32 devices in a mesh: sp: 8 (over z, x), tp: 4 (over y, core).
Axes of the slice: x: 2, y: 2, z: 4, core: 2. Of those that a mesh axis runs over, the one named last changes fastest.
Arguments:
- glu_value: bfloat16 [1536, 1024], P('sp', 'tp'), may hold values from -6 to 6
- glu_gate: bfloat16 [1536, 1024], P('sp', 'tp'), may hold values from -6 to 6
- doc_ids: int32 [1536], P('sp'), may hold values from 0 to 3, never falling along the last dimension, each value on 1 to 768 neighbouring positions
- conv_kernel: bfloat16 [31, 1024], P(None, 'tp')
- conv_gain: float32 [1024], P('tp'), may hold values from 0.1 to 1.9
- out_weight: bfloat16 [1024, 2048], P('tp'), may hold values from -0.1875 to 0.1875
- residual: bfloat16 [1536, 2048], P('sp'), may hold values from -6 to 6
- mix_gain: float32 [2048], replicated, may hold values from 0.1 to 1.9
- routes: int32 [1536, 2], P('sp'), may hold values from 0 to 7, all different within a row; in each aligned block of 192 rows (0 to 191, 192 to 383, ...) at most 96 rows name the same one
- route_weights: float32 [1536, 2], P('sp'), may hold values from 0.2 to 1
- expert_gate: bfloat16 [8, 2048, 5120], P('sp', None, 'tp'), may hold values from -0.125 to 0.125
- expert_up: bfloat16 [8, 2048, 5120], P('sp', None, 'tp'), may hold values from -0.125 to 0.125
- expert_down: bfloat16 [8, 5120, 2048], P('sp', 'tp')
- final_gain: float32 [2048], P('tp'), may hold values from 0.1 to 1.9
Outputs:
- block_out: bfloat16 [1536, 2048], P('sp', 'tp')
The draws below stay inside these ranges and needn't reach their ends.
Inputs may be any that keep to these rules, and one draw needn't show every extreme that they name: `routes`: each row names two different experts. In each aligned block of 192 rows no expert is named by more than 96 rows, and in every draw some block has an expert named by exactly 96 rows. `doc_ids`: document numbers never fall along the sequence.
All inputs are finite; a program needn't handle non-finite values.
Results may differ from the reference program's by a relative error of at most 0.022.
Values may be sent and summed in bfloat16 or wider, within the bound.
A program may use at most 64 MiB of HBM per device.

```python
import math
import jax
import jax.numpy as jnp
import numpy as np
from jax import lax

D = 2048
C = 1024
FF = 5120
WIDTH = 31
TOK = 192
EXPERTS = 8
TOKENS = 1536
CAP = 96
DOCS = 4
DOC_MOST = 768
N_SP = 8
N_TP = 4


def draw_conv_kernel(key, part):
    base_draw = jax.random.normal(key, (WIDTH, C), jnp.float32)
    ramp_scale = jnp.exp(jnp.log(4.0) * jnp.arange(C, dtype=jnp.float32) / C)[None, :]
    return (base_draw * ramp_scale * WIDTH ** (-0.5)).astype(jnp.bfloat16)


def draw_expert_down(key, part):
    ramp_scale = jnp.exp(jnp.log(4.0) * (jnp.arange(D, dtype=jnp.float32) / D - 0.5))[None, None, :]
    base_draw = jax.random.normal(key, (EXPERTS, FF, D), jnp.float32)
    return (base_draw * ramp_scale * FF ** (-0.5)).astype(jnp.bfloat16)


def steps_of(stream_key, dims, cuts, least, top_value):
    level = 1.0
    for dim, shards_of in cuts:
        steps = jax.random.uniform(jax.random.fold_in(jax.random.fold_in(stream_key, 6), dim), (shards_of,), jnp.float32, least / len(cuts), top_value / len(cuts))
        level = level * jnp.repeat(jnp.exp(steps), dims[dim] // shards_of).reshape((-1,) + (1,) * (len(dims) - 1 - dim))
    return level


def profile(amount, total, reach, skew):
    weights = [(1 << 20) // math.isqrt(grade ** skew) + 1 for grade in range(2, amount + 1)]
    surplus, counts = total - reach - (amount - 1), [1] * (amount - 1)
    while surplus > 0:
        movable = [i for i in range(amount - 1) if counts[i] < reach]
        pool, left = sum([weights[i] for i in movable]), surplus
        for i in movable:
            addition = min(reach - counts[i], max(1, left * weights[i] // pool), surplus)
            counts[i] = counts[i] + addition
            surplus = surplus - addition
    return np.array([reach] + counts)


def uneven(key, number_of, total, most, skew):
    if number_of == 2:
        one = jax.random.randint(key, (), max(1, total - most), min(most, total - 1) + 1)
        return jnp.stack([one, total - one])
    sizes = jnp.asarray(profile(number_of, total, most, skew), jnp.int32)
    pairs = (number_of - 1) // 2
    giver, receiver = sizes[1:1 + 2 * pairs:2], sizes[2:2 + 2 * pairs:2]
    slack = jnp.minimum(giver - 1, most - receiver)
    shifted = jax.random.randint(jax.random.fold_in(key, 1), (pairs,), 0, 1 << 20) % (slack + 1)
    sizes = sizes.at[1:1 + 2 * pairs:2].set(giver - shifted).at[2:2 + 2 * pairs:2].set(receiver + shifted)
    return sizes[jax.random.permutation(jax.random.fold_in(key, 2), number_of)]


def shared_out(rng, own, number, rows, number_of, top, limit, lean):
    sequence = jax.random.permutation(rng, number_of)
    heavy_load, common = portions_of(number_of, rows * top, limit, lean, True), portions_of(number_of, rows * top, limit, lean, False)
    places = jnp.arange(number_of)

    def named(lengths, rotation):
        used = int((lengths > 0).sum())
        fixed = max(1, used // 4)
        moved = fixed + (places - fixed + rotation * (used - fixed)) % max(1, number_of - fixed)
        return jnp.zeros((number_of,), jnp.int32).at[sequence[jnp.where(places < fixed, places, moved)]].set(jnp.asarray(lengths, jnp.int32))

    lengths = jnp.where(number % 4 == 0, named(heavy_load, number // 4), named(common, number - number // 4 - 1))
    mixed = jax.random.permutation(jax.random.fold_in(own, 3), number_of)
    giver, sink = mixed[0:number_of // 2 * 2:2], mixed[1:number_of // 2 * 2:2]
    room = jnp.minimum(lengths[giver] - 1, limit - lengths[sink]) // 2
    room = jnp.where((giver == sequence[0]) | (sink == sequence[0]) | (lengths[sink] == 0), 0, jnp.maximum(room, 0))
    moved = jax.random.randint(jax.random.fold_in(own, 4), (number_of // 2,), 0, 1 << 20) % (room + 1)
    lengths = lengths.at[giver].add(-moved).at[sink].add(moved)
    members = jnp.searchsorted(jnp.cumsum(lengths), jnp.arange(rows * top), side="right").astype(jnp.int32)
    grid = members.reshape(top, rows).T
    grid = grid[jax.random.permutation(jax.random.fold_in(own, 1), rows)]
    rotation = jax.random.randint(jax.random.fold_in(own, 2), (rows, 1), 0, top)
    return jnp.take_along_axis(grid, (jnp.arange(top)[None, :] + rotation) % top, axis=1)


def portions_of(amount, total, most, slope, full):
    loads = [(1 << 20) // math.isqrt(grade ** slope) + 1 for grade in range(1, amount + 1)]
    largest = most if full else min(most, max(-(-total // amount), total * loads[0] // sum(loads)))
    least = 1 if total - largest >= amount - 1 else 0
    counts, spare = [largest] + [least] * (amount - 1), total - largest - least * (amount - 1)
    while spare > 0:
        movable = [i for i in range(1, amount) if counts[i] < largest] or [i for i in range(1, amount) if counts[i] < most]
        pool, budget = sum([loads[i] for i in movable]), spare
        for i in movable:
            more = min(most - counts[i], max(1, budget * loads[i] // pool), spare)
            counts[i] = counts[i] + more
            spare = spare - more
    return np.array(counts)


def bell_draw(key, extent, spread, bound, split=(), kind=jnp.bfloat16):
    drawn = jax.random.normal(key, extent, jnp.float32) * spread
    if len(split) > 0:
        drawn = steps_of(key, extent, split, -0.22, 0.18) * drawn
    return jnp.clip(drawn, min=-bound, max=bound).astype(kind)


def setup_inputs(seed: int = 0) -> dict:
    splits = jax.random.split(jax.random.key(seed), 15)
    glu_value = bell_draw(splits[0], (TOKENS, C), 1.0, 6.0, ((0, 8), (1, 4)))
    glu_gate = bell_draw(splits[1], (TOKENS, C), 1.0, 6.0, ((0, 8), (1, 4)))
    doc_ids = jnp.searchsorted(jnp.cumsum(uneven(splits[2], DOCS, TOKENS, DOC_MOST, 1)), jnp.arange(TOKENS), side="right").astype(jnp.int32)
    conv_kernel = draw_conv_kernel(jax.random.fold_in(splits[14], 71), 0)
    conv_gain = jnp.clip(1.0 + 0.18 * jax.random.normal(splits[4], (C,), jnp.float32), 0.1, 1.9)
    out_weight = bell_draw(splits[5], (C, D), C ** -0.5, 0.1875, ((0, 4),))
    residual = bell_draw(splits[6], (TOKENS, D), 1.0, 6.0, ((0, 8),))
    mix_gain = jnp.clip(1.0 + 0.18 * jax.random.normal(splits[7], (D,), jnp.float32), 0.1, 1.9)
    routes_keys = jax.random.split(jax.random.fold_in(splits[8], 1), TOKENS // TOK)
    routes_turns = jax.random.permutation(jax.random.fold_in(splits[8], 3), TOKENS // TOK)
    routes = jax.vmap(lambda own, number: shared_out(jax.random.fold_in(splits[8], 2), own, number, TOK, EXPERTS, 2, CAP, 2))(routes_keys, routes_turns).reshape((TOKENS, 2))
    route_weights = jnp.clip(0.2 + 0.8 * jax.random.uniform(splits[9], (TOKENS, 2), jnp.float32) ** steps_of(splits[9], (TOKENS, 2), ((0, 8),), -0.2, 0.2), 0.2, 1.0)
    expert_gate = bell_draw(splits[10], (EXPERTS, D, FF), D ** -0.5, 0.125, ((0, 8), (2, 4)))
    expert_up = bell_draw(splits[11], (EXPERTS, D, FF), D ** -0.5, 0.125, ((0, 8), (2, 4)))
    expert_down = draw_expert_down(jax.random.fold_in(splits[14], 71), 0)
    final_gain = jnp.clip(1.0 + 0.18 * jax.random.normal(splits[13], (D,), jnp.float32), 0.1, 1.9)
    return {"glu_value": glu_value, "glu_gate": glu_gate, "doc_ids": doc_ids, "conv_kernel": conv_kernel, "conv_gain": conv_gain, "out_weight": out_weight, "residual": residual, "mix_gain": mix_gain, "routes": routes, "route_weights": route_weights, "expert_gate": expert_gate, "expert_up": expert_up, "expert_down": expert_down, "final_gain": final_gain}


residual_alpha = 1.41421356
norm_eps = 1e-05

def scaled_norm(pre_norm, gain):
    row_mean = lax.optimization_barrier(jnp.mean(pre_norm, -1, keepdims=True))
    row_var = lax.optimization_barrier(jnp.mean(pre_norm * pre_norm, -1, keepdims=True)) - row_mean * row_mean
    return (pre_norm - row_mean) * lax.rsqrt(row_var + norm_eps) * gain

def reference(glu_value, glu_gate, doc_ids, conv_kernel, conv_gain, out_weight, residual, mix_gain, routes, route_weights, expert_gate, expert_up, expert_down, final_gain):
    seq_len = glu_value.shape[0]
    gated_rows = (glu_value.astype(jnp.float32) * jax.nn.sigmoid(glu_gate.astype(jnp.float32))).astype(jnp.bfloat16)
    gated_wide = gated_rows.astype(jnp.float32)
    kernel = conv_kernel.astype(jnp.float32)
    filtered = jnp.zeros(gated_wide.shape, jnp.float32)
    for shift_by in range(WIDTH):
        moved_rows = jnp.pad(gated_wide, ((shift_by, 0), (0, 0)))[:seq_len]
        moved_ids = jnp.pad(doc_ids, (shift_by, 0), constant_values=-1)[:seq_len]
        same_doc = (moved_ids == doc_ids)[:, None]
        filtered = filtered + jnp.where(same_doc, moved_rows, 0.0) * kernel[shift_by]
    conv_out = jax.nn.silu(scaled_norm(filtered, conv_gain.astype(jnp.float32))).astype(jnp.bfloat16)
    width_block = C // N_TP
    mix_total = jnp.zeros((seq_len, D), jnp.float32)
    for block_at in range(N_TP):
        columns = conv_out[:, block_at * width_block:(block_at + 1) * width_block]
        weights = out_weight[block_at * width_block:(block_at + 1) * width_block]
        mix_total = mix_total + jnp.dot(columns, weights, preferred_element_type=jnp.float32).astype(jnp.bfloat16).astype(jnp.float32)
    mixed_rows = scaled_norm(residual_alpha * residual.astype(jnp.float32) + mix_total, mix_gain.astype(jnp.float32)).astype(jnp.bfloat16)
    chosen = routes.reshape(N_SP, TOK * 2)
    member = (chosen[:, :, None] == jnp.arange(EXPERTS, dtype=jnp.int32)[None, None, :]).astype(jnp.int32)
    earlier = jnp.cumsum(member, 1) - member
    rank_in = lax.optimization_barrier(jnp.sum(earlier * member, -1))
    group_at = jnp.arange(N_SP, dtype=jnp.int32)[:, None]
    row_at = (group_at * CAP + rank_in).reshape(-1).astype(jnp.int32)
    expert_at = chosen.reshape(-1).astype(jnp.int32)
    token_at = jnp.repeat(jnp.arange(seq_len, dtype=jnp.int32), 2)
    expert_inbox = jnp.zeros((EXPERTS, N_SP * CAP, D), jnp.bfloat16).at[expert_at, row_at].set(mixed_rows[token_at])
    hidden_block = FF // N_TP

    def run_expert(packed):
        in_rows, w_gate, w_up, w_down = packed
        gate_proj = jnp.dot(in_rows, w_gate, preferred_element_type=jnp.float32)
        up_proj = jnp.dot(in_rows, w_up, preferred_element_type=jnp.float32)
        hidden = (jax.nn.silu(gate_proj) * up_proj).astype(jnp.bfloat16)
        running = jnp.zeros((in_rows.shape[0], D), jnp.float32)
        for block_at in range(N_TP):
            piece_out = jnp.dot(hidden[:, block_at * hidden_block:(block_at + 1) * hidden_block], w_down[block_at * hidden_block:(block_at + 1) * hidden_block], preferred_element_type=jnp.float32)
            running = running + piece_out.astype(jnp.bfloat16).astype(jnp.float32)
        return running.astype(jnp.bfloat16)
    expert_outbox = lax.map(run_expert, (expert_inbox, expert_gate, expert_up, expert_down))
    picked = expert_outbox[expert_at, row_at].astype(jnp.float32).reshape(seq_len, 2, D)
    moe_sum = lax.optimization_barrier(jnp.sum(route_weights[:, :, None] * picked, 1))
    pre_norm = residual_alpha * mixed_rows.astype(jnp.float32) + moe_sum
    return scaled_norm(pre_norm, final_gain.astype(jnp.float32)).astype(jnp.bfloat16)
```

```python
import functools

import jax
import jax.numpy as jnp
from jax import lax
from jax.experimental import pallas as pl
from jax.experimental.pallas import tpu as pltpu
from jax.sharding import PartitionSpec as P

residual_alpha = 1.41421356
norm_eps = 1e-05


def from_behind(value, axis, by):
    peers = lax.axis_size(axis)
    pairs = [(i, i + by) for i in range(peers) if 0 <= i + by < peers]
    return lax.ppermute(value, axis, pairs)


def scaled_norm(pre_norm, gain):
    row_mean = jnp.mean(pre_norm, -1, keepdims=True)
    row_var = jnp.mean(pre_norm * pre_norm, -1, keepdims=True) - row_mean * row_mean
    return (pre_norm - row_mean) * lax.rsqrt(row_var + norm_eps) * gain


def local_plain(
    glu_value,
    glu_gate,
    doc_ids,
    conv_kernel,
    conv_gain,
    out_weight,
    residual,
    mix_gain,
    routes,
    route_weights,
    expert_gate,
    expert_up,
    expert_down,
    final_gain,
):
    tok_rows = glu_value.shape[0]
    rim_len = conv_kernel.shape[0] - 1
    channels = glu_value.shape[1] * lax.axis_size("tp")
    gated_rows = (
        glu_value.astype(jnp.float32) * jax.nn.sigmoid(glu_gate.astype(jnp.float32))
    ).astype(jnp.bfloat16)
    rim_rows, rim_ids = from_behind(
        (gated_rows[tok_rows - rim_len :], doc_ids[tok_rows - rim_len :]), "sp", 1
    )
    extended = jnp.concatenate([rim_rows, gated_rows], 0).astype(jnp.float32)
    ext_ids = jnp.concatenate([rim_ids, doc_ids], 0)
    kernel = conv_kernel.astype(jnp.float32)
    filtered = jnp.zeros(gated_rows.shape, jnp.float32)
    for shift_by in range(rim_len + 1):
        begin_at = rim_len - shift_by
        same_doc = (ext_ids[begin_at : begin_at + tok_rows] == doc_ids)[:, None]
        filtered = (
            filtered
            + jnp.where(same_doc, extended[begin_at : begin_at + tok_rows], 0.0) * kernel[shift_by]
        )
    row_sum, row_square = lax.psum((jnp.sum(filtered, 1), jnp.sum(filtered * filtered, 1)), "tp")
    row_mean = row_sum[:, None] / channels
    row_var = row_square[:, None] / channels - row_mean * row_mean
    conv_out = jax.nn.silu(
        (filtered - row_mean) * lax.rsqrt(row_var + norm_eps) * conv_gain
    ).astype(jnp.bfloat16)
    mix_total = lax.psum(
        jnp.dot(conv_out, out_weight, preferred_element_type=jnp.float32).astype(jnp.bfloat16), "tp"
    ).astype(jnp.float32)
    mixed_rows = scaled_norm(
        residual_alpha * residual.astype(jnp.float32) + mix_total, mix_gain
    ).astype(jnp.bfloat16)
    experts = expert_gate.shape[0] * lax.axis_size("sp")
    capacity = 4 * tok_rows // experts
    chosen = routes.reshape(-1)
    member = (chosen[:, None] == jnp.arange(experts, dtype=jnp.int32)[None, :]).astype(jnp.int32)
    earlier = jnp.cumsum(member, 0) - member
    slot_index = chosen * capacity + jnp.sum(earlier * member, 1)
    dispatch_table = jnp.any(
        jnp.arange(experts * capacity, dtype=jnp.int32)[:, None, None]
        == slot_index.reshape(tok_rows, 2)[None],
        -1,
    ).astype(jnp.bfloat16)
    feat_block = mixed_rows.shape[1] // lax.axis_size("tp")
    offset = lax.axis_index("tp") * feat_block
    w_gate = expert_gate[0]
    w_up = expert_up[0]
    w_down = expert_down[0]
    row_slice = lax.dynamic_slice_in_dim(mixed_rows, offset, feat_block, 1)
    outgoing = (
        jnp.dot(dispatch_table, row_slice, preferred_element_type=jnp.float32)
        .astype(jnp.bfloat16)
        .reshape(experts, capacity, feat_block)
    )
    arrived = lax.all_to_all(outgoing, "sp", split_axis=0, concat_axis=0, tiled=True)
    sources, slot_count, part_width = arrived.shape
    flat_rows = arrived.reshape(sources * slot_count, part_width)
    col_piece = lax.all_gather(flat_rows, "tp", axis=1, tiled=True)
    gate_proj = jnp.dot(col_piece, w_gate, preferred_element_type=jnp.float32)
    up_proj = jnp.dot(col_piece, w_up, preferred_element_type=jnp.float32)
    hidden = (jax.nn.silu(gate_proj) * up_proj).astype(jnp.bfloat16)
    partial_value = jnp.dot(hidden, w_down, preferred_element_type=jnp.float32).reshape(
        sources, slot_count, -1
    )
    summed = lax.psum_scatter(
        partial_value.astype(jnp.bfloat16), "tp", scatter_dimension=2, tiled=True
    )
    returned = lax.all_to_all(summed, "sp", split_axis=0, concat_axis=0, tiled=True)
    flat_back = returned.reshape(experts * capacity, feat_block)
    picked = flat_back[slot_index].astype(jnp.float32).reshape(tok_rows, 2, feat_block)
    moe_sum = jnp.sum(route_weights[:, :, None] * picked, 1)
    own_cols = lax.dynamic_slice_in_dim(mixed_rows, offset, feat_block, 1).astype(jnp.float32)
    pre_norm = residual_alpha * own_cols + moe_sum
    fin_sum, fin_square = lax.psum((jnp.sum(pre_norm, 1), jnp.sum(pre_norm * pre_norm, 1)), "tp")
    features = feat_block * lax.axis_size("tp")
    fin_mean = fin_sum[:, None] / features
    fin_var = fin_square[:, None] / features - fin_mean * fin_mean
    return ((pre_norm - fin_mean) * lax.rsqrt(fin_var + norm_eps) * final_gain).astype(jnp.bfloat16)


HALO = 32
PAIR = 2
TILE = 256
F32 = jnp.float32
BF16 = jnp.bfloat16


def block_kernel(
    sp_n,
    tp_n,
    capacity,
    taps,
    glu_value,
    glu_gate,
    ids_row,
    conv_kernel,
    conv_gain,
    out_weight_hbm,
    residual_hbm,
    mix_gain,
    routes_row,
    weights_row,
    gate_hbm,
    up_hbm,
    down_hbm,
    final_gain,
    out,
    w_out,
    resid,
    w_gate,
    w_up,
    w_down,
    rim_out,
    rim_in,
    rim_ids,
    by_row,
    by_col,
    ext,
    ext_ids,
    fil,
    stat_out,
    stat_in,
    mix_pp,
    mix_a,
    mix_s,
    mix_b,
    mixed,
    outbox,
    rows_in,
    hidden,
    part_pp,
    part_a,
    part_s,
    part_b,
    part_own,
    back_out,
    back_in,
    load_sem,
    halo_sem,
    stat_send,
    stat_recv,
    mix_send,
    mix_recv,
    disp_send,
    disp_recv,
    ag_send,
    ag_recv,
    part_send,
    part_recv,
    cross_send,
    cross_recv,
    back_send,
    back_recv,
):
    tok = glu_value.shape[0]
    chan = glu_value.shape[1]
    feat = final_gain.shape[1]
    ff = hidden.shape[2]
    y_n = tp_n // 2
    sp = lax.axis_index("sp")
    tp = lax.axis_index("tp")
    y = tp // 2
    core = tp % 2
    partner = y * 2 + (1 - core)
    groups = sp_n // PAIR
    group_rows = PAIR * capacity
    pending = []

    def y_at(k):
        return lax.rem(y + k, y_n)

    near = list(range(PAIR, sp_n // 2))
    far = sorted(range(sp_n // 2, sp_n), key=lambda r: (r % 2, r))
    rest = [(2 * i + 1) / len(far) for i in range(len(far))], [(2 * i + 1) / len(near) for i in range(len(near))]
    turns = list(range(PAIR)) + [r for _, r in sorted(zip(rest[0] + rest[1], far + near))]

    def peer(p):
        to, bit = sp, 1
        while bit < sp_n:
            if turns[p] & bit:
                to = to + bit - 2 * bit * lax.rem(lax.div(sp, bit), 2)
            bit *= 2
        return to

    def feat_cols(block):
        return pl.ds(pl.multiple_of(block * feat, feat), feat)

    def remote(src, dst, send, recv, axis, to):
        return pltpu.make_async_remote_copy(
            src_ref=src,
            dst_ref=dst,
            send_sem=send,
            recv_sem=recv,
            device_id={axis: to},
            device_id_type=pl.DeviceIdType.MESH,
        )

    def send(*args):
        copy = remote(*args)
        copy.start()
        pending.append(copy)

    def arrived(dst, recv, send_sem, axis, to):
        remote(dst, dst, send_sem, recv, axis, to).wait_recv()

    loads = []
    for i, (src, dst) in enumerate(
        (
            (out_weight_hbm, w_out),
            (residual_hbm.at[:, feat_cols(tp)], resid),
            (gate_hbm.at[0], w_gate),
            (up_hbm.at[0], w_up),
            (down_hbm.at[0], w_down),
        )
    ):
        copy = pltpu.make_async_copy(src, dst, load_sem.at[i])
        copy.start()
        loads.append(copy)

    barrier = pltpu.get_barrier_semaphore()
    for k in range(1, sp_n):
        pl.semaphore_signal(
            barrier, inc=1, device_id={"sp": lax.rem(sp + k, sp_n)},
            device_id_type=pl.DeviceIdType.MESH,
        )
    for k in range(1, tp_n):
        pl.semaphore_signal(
            barrier, inc=1, device_id={"tp": lax.rem(tp + k, tp_n)},
            device_id_type=pl.DeviceIdType.MESH,
        )

    lanes = 128
    wide = by_row.shape[1]
    by_row[...] = jnp.zeros_like(by_row)
    by_row[0:1, 0:tok] = ids_row[...].astype(F32)
    by_row[1:3, 0:tok] = routes_row[...].astype(F32)
    by_row[3:5, 0:tok] = weights_row[...]
    by_col[...] = jnp.concatenate([by_row[...], jnp.zeros((lanes - 8, wide), F32)], 0).T[:tok]
    ext_ids[HALO:, :] = jnp.broadcast_to(by_col[:, 0:1].astype(jnp.int32), (tok, lanes))

    value = glu_value[...].astype(F32)
    gated = (value * jax.nn.sigmoid(glu_gate[...].astype(F32))).astype(BF16)
    ext[HALO:, :] = gated.astype(F32)
    rim_out[...] = gated[tok - HALO :]

    lower = (
        lax.broadcasted_iota(jnp.int32, (tok, tok), 1)
        < lax.broadcasted_iota(jnp.int32, (tok, tok), 0)
    )
    upper = (
        lax.broadcasted_iota(jnp.int32, (tok, tok), 0)
        < lax.broadcasted_iota(jnp.int32, (tok, tok), 1)
    )
    e_lane = lax.broadcasted_iota(jnp.int32, (tok, lanes), 1)
    one_lane = lax.broadcasted_iota(jnp.int32, (1, lanes), 1)
    subs = -(-sp_n // 16) * 16
    e_sub = lax.broadcasted_iota(jnp.int32, (subs, tok), 0)
    lane_expert = jnp.full((1, lanes), -1, jnp.int32)
    sub_expert = jnp.full((subs, tok), -1, jnp.int32)
    for r in range(sp_n):
        lane_expert = jnp.where(one_lane == r, peer(r), lane_expert)
        sub_expert = jnp.where(e_sub == r, peer(r), sub_expert)
    lane_expert = lane_expert.astype(F32)
    m0 = (by_col[:, 1:2] == lane_expert).astype(F32)
    m1 = (by_col[:, 2:3] == lane_expert).astype(F32)
    rank = jnp.dot(lower.astype(F32).astype(BF16), (m0 + m1).astype(BF16), preferred_element_type=F32)
    place = rank + (e_lane * capacity).astype(F32)
    slot_col0 = jnp.sum(m0 * place, 1, keepdims=True).astype(jnp.int32)
    slot_col1 = jnp.sum(m1 * place, 1, keepdims=True).astype(jnp.int32)
    n0 = (routes_row[0:1, :] == sub_expert).astype(F32)
    n1 = (routes_row[1:2, :] == sub_expert).astype(F32)
    rank_r = jnp.dot((n0 + n1).astype(BF16), upper.astype(F32).astype(BF16), preferred_element_type=F32)
    place_r = rank_r + (e_sub * capacity).astype(F32)
    slot_row0 = jnp.sum(n0 * place_r, 0, keepdims=True).astype(jnp.int32)
    slot_row1 = jnp.sum(n1 * place_r, 0, keepdims=True).astype(jnp.int32)

    pl.semaphore_wait(barrier, sp_n + tp_n - 2)

    right = lax.rem(sp + 1, sp_n)
    halo = [
        remote(src, dst, halo_sem.at[0, i], halo_sem.at[1, i], "sp", right)
        for i, (src, dst) in enumerate(
            ((rim_out, rim_in), (ext_ids.at[pl.ds(tok, HALO)], rim_ids))
        )
    ]

    @pl.when(sp < sp_n - 1)
    def _():
        for copy in halo:
            copy.start()

    kern = conv_kernel[...].astype(F32)
    lane_blocks = chan // lanes

    def convolve(at):
        own = ext_ids[HALO + at : 2 * HALO + at, :]
        acc = [jnp.zeros((HALO, lanes), F32) for _ in range(lane_blocks)]
        for lag in range(taps):
            begin = HALO + at - lag
            same = ext_ids[begin : begin + HALO, :] == own
            for b in range(lane_blocks):
                part = ext[begin : begin + HALO, b * lanes : (b + 1) * lanes]
                acc[b] = acc[b] + jnp.where(same, part, 0.0) * kern[lag : lag + 1, b * lanes : (b + 1) * lanes]
        for b in range(lane_blocks):
            fil[at : at + HALO, b * lanes : (b + 1) * lanes] = acc[b]

    for at in range(HALO, tok, HALO):
        convolve(at)

    @pl.when(sp == 0)
    def _():
        ext[:HALO, :] = jnp.zeros((HALO, chan), F32)
        ext_ids[:HALO, :] = jnp.full((HALO, lanes), -1, jnp.int32)

    @pl.when(sp > 0)
    def _():
        for copy in halo:
            copy.wait_recv()
        ext[:HALO, :] = rim_in[...].astype(F32)
        ext_ids[:HALO, :] = rim_ids[...]

    convolve(0)

    def stats(i, value, width):
        row_sum = jnp.sum(value, 1, keepdims=True)
        row_square = jnp.sum(value * value, 1, keepdims=True)
        packed = jnp.where(e_lane == 0, row_sum, jnp.where(e_lane == 1, row_square, 0.0))
        packed = jnp.concatenate([packed, jnp.zeros((wide - tok, lanes), F32)], 0)
        stat_out[i] = packed.T[:8]
        for k in range(1, tp_n):
            send(
                stat_out.at[i], stat_in.at[i, k], stat_send.at[i, k], stat_recv.at[i, k],
                "tp", lax.rem(tp + k, tp_n),
            )
        total = stat_out[i]
        for k in range(1, tp_n):
            arrived(stat_in.at[i, k], stat_recv.at[i, k], stat_send.at[i, k], "tp", partner)
            total = total + stat_in[i, k]
        total = jnp.concatenate([total, jnp.zeros((lanes - 8, wide), F32)], 0).T[:tok]
        mean = total[:, 0:1] / width
        var = total[:, 1:2] / width - mean * mean
        return mean, lax.rsqrt(var + norm_eps)

    filtered = fil[...]
    mean, scale = stats(0, filtered, chan * tp_n)
    normed = (filtered - mean) * scale * conv_gain[...]
    conv_out = (normed * jax.nn.sigmoid(normed)).astype(BF16)

    loads[0].wait()
    order = list(range(1, y_n)) + [0]
    for k in order:
        cols = feat_cols(2 * y_at(k) + 1 - core)
        mix_pp[k] = jnp.dot(conv_out, w_out[:, cols], preferred_element_type=F32).astype(BF16)
        send(mix_pp.at[k], mix_a.at[k], mix_send.at[0, k], mix_recv.at[0, k], "tp", partner)
    own_mix = None
    for k in order:
        cols = feat_cols(2 * y_at(k) + core)
        value = jnp.dot(conv_out, w_out[:, cols], preferred_element_type=F32)
        arrived(mix_a.at[k], mix_recv.at[0, k], mix_send.at[0, k], "tp", partner)
        value = value + mix_a[k].astype(F32)
        if k:
            mix_s[k] = value.astype(BF16)
            send(
                mix_s.at[k], mix_b.at[k], mix_send.at[1, k], mix_recv.at[1, k],
                "tp", 2 * y_at(k) + core,
            )
        else:
            own_mix = value
    loads[1].wait()
    pre = own_mix + residual_alpha * resid[...].astype(F32)
    for k in range(1, y_n):
        arrived(mix_b.at[k], mix_recv.at[1, k], mix_send.at[1, k], "tp", partner)
        pre = pre + mix_b[k].astype(F32)
    mean, scale = stats(1, pre, feat * tp_n)
    mixed[...] = ((pre - mean) * scale * mix_gain[:, feat_cols(tp)]).astype(BF16)

    def spread(d):
        block = rows_in.at[tp, d]
        send(block, block, ag_send.at[0, d], ag_recv.at[0, d], "tp", partner)
        for k in range(1, y_n):
            send(
                block, block, ag_send.at[k, d], ag_recv.at[k, d],
                "tp", 2 * y_at(k) + core,
            )

    def pass_on(d):
        for k in range(1, y_n):
            block = rows_in.at[2 * y_at(y_n - k) + core, d]
            arrived(block, ag_recv.at[k, d], ag_send.at[k, d], "tp", partner)
            send(
                block, block, ag_send.at[y_n - 1 + k, d], ag_recv.at[y_n - 1 + k, d],
                "tp", partner,
            )

    def gathered(d):
        block = rows_in.at[partner, d]
        arrived(block, ag_recv.at[0, d], ag_send.at[0, d], "tp", partner)
        for k in range(1, y_n):
            block = rows_in.at[2 * y_at(y_n - k) + 1 - core, d]
            arrived(block, ag_recv.at[y_n - 1 + k, d], ag_send.at[y_n - 1 + k, d], "tp", partner)

    def dispatch(p):
        s_at = lax.broadcasted_iota(jnp.int32, (capacity, tok), 0) + p * capacity
        table = jnp.logical_or(s_at == slot_row0, s_at == slot_row1).astype(F32).astype(BF16)
        block = jnp.dot(table, mixed[...], preferred_element_type=F32).astype(BF16)
        if p:
            outbox[p] = block
            send(
                outbox.at[p], rows_in.at[tp, p], disp_send.at[p], disp_recv.at[p],
                "sp", peer(p),
            )
        else:
            rows_in[tp, 0] = block
            spread(0)

    def landed(p):
        arrived(rows_in.at[tp, p], disp_recv.at[p], disp_send.at[p], "sp", right)
        spread(p)

    def gate_up(g, n):
        cols = pl.ds(n * TILE, TILE)
        rows = [
            rows_in[j, PAIR * g : PAIR * (g + 1)].reshape(group_rows, feat) for j in range(tp_n)
        ]
        x = jnp.concatenate(rows, 1)
        gate = jnp.dot(x, w_gate[:, cols], preferred_element_type=F32)
        up = jnp.dot(x, w_up[:, cols], preferred_element_type=F32)
        hidden[g, :, cols] = (gate * jax.nn.sigmoid(gate) * up).astype(BF16)

    def down(g):
        def part(block):
            return jnp.dot(hidden[g], w_down[:, feat_cols(block)], preferred_element_type=F32)

        for k in order:
            part_pp[g, k] = part(2 * y_at(k) + 1 - core).astype(BF16)
            send(
                part_pp.at[g, k], part_a.at[g, k], part_send.at[g, k], part_recv.at[g, k],
                "tp", partner,
            )
            part_own[g, k] = part(2 * y_at(k) + core)

    def cross(g):
        for k in order[:-1]:
            arrived(part_a.at[g, k], part_recv.at[g, k], part_send.at[g, k], "tp", partner)
            part_s[g, k] = (part_own[g, k] + part_a[g, k].astype(F32)).astype(BF16)
            for i in range(PAIR):
                rows = pl.ds(i * capacity, capacity)
                send(
                    part_s.at[g, k, rows], part_b.at[g, k, rows],
                    cross_send.at[g, k, i], cross_recv.at[g, k, i],
                    "tp", 2 * y_at(k) + core,
                )
        arrived(part_a.at[g, 0], part_recv.at[g, 0], part_send.at[g, 0], "tp", partner)

    def finish(p):
        g, i = p // PAIR, p % PAIR
        rows = pl.ds(i * capacity, capacity)
        value = part_own[g, 0, rows, :] + part_a[g, 0, rows, :].astype(F32)
        for k in range(1, y_n):
            arrived(
                part_b.at[g, k, rows], cross_recv.at[g, k, i], cross_send.at[g, k, i],
                "tp", partner,
            )
            value = value + part_b[g, k, rows, :].astype(F32)
        if p:
            back_out[p] = value.astype(BF16)
            send(
                back_out.at[p], back_in.at[p], back_send.at[p], back_recv.at[p],
                "sp", peer(p),
            )
        else:
            back_in[0] = value.astype(BF16)

    tiles = ff // TILE
    early = PAIR + 3
    for p in range(early):
        dispatch(p)
    pass_on(0)
    for p in range(early, sp_n):
        dispatch(p)
    landed(1)
    landed(2)
    pass_on(1)
    loads[2].wait()
    loads[3].wait()
    for g in range(groups):
        for p in range(PAIR * g, PAIR * (g + 1)):
            gathered(p)
        gaps = -(-tiles // 2)
        steps = [[] for _ in range(gaps + 1)]

        def put(gap, step, p):
            if p < sp_n:
                steps[min(gap, gaps)].append(functools.partial(step, p))

        put(0, landed, PAIR * g + 3)
        put(1, pass_on, PAIR * g + 2)
        put(1, landed, PAIR * g + 4)
        put(gaps, pass_on, PAIR * g + 3)
        if g >= 2:
            put(1, finish, PAIR * (g - 2))
            put(2, finish, PAIR * (g - 2) + 1)
        for n in range(tiles):
            gate_up(g, n)
            if n % 2 or n == tiles - 1:
                for step in steps[n // 2]:
                    step()
        if g == 0:
            loads[4].wait()
        down(g)
        cross(g)
        for step in steps[gaps]:
            step()
    for g in range(groups - 2, groups):
        for i in range(PAIR):
            finish(PAIR * g + i)

    for p in range(1, sp_n):
        arrived(back_in.at[p], back_recv.at[p], back_send.at[p], "sp", right)
    slots = sp_n * capacity
    returned = back_in[...].reshape(slots, feat)
    s_lane = lax.broadcasted_iota(jnp.int32, (tok, slots), 1)
    pick0 = jnp.dot((s_lane == slot_col0).astype(F32).astype(BF16), returned, preferred_element_type=F32)
    pick1 = jnp.dot((s_lane == slot_col1).astype(F32).astype(BF16), returned, preferred_element_type=F32)
    moe = by_col[:, 3:4] * pick0 + by_col[:, 4:5] * pick1
    pre = residual_alpha * mixed[...].astype(F32) + moe
    mean, scale = stats(2, pre, feat * tp_n)
    out[...] = ((pre - mean) * scale * final_gain[...]).astype(BF16)
    for copy in pending:
        copy.wait_send()

    @pl.when(sp < sp_n - 1)
    def _():
        for copy in halo:
            copy.wait_send()


def local_kernel(
    glu_value,
    glu_gate,
    doc_ids,
    conv_kernel,
    conv_gain,
    out_weight,
    residual,
    mix_gain,
    routes,
    route_weights,
    expert_gate,
    expert_up,
    expert_down,
    final_gain,
):
    sp_n, tp_n = lax.axis_size("sp"), lax.axis_size("tp")
    tok, chan = glu_value.shape
    feat = final_gain.shape[0]
    width, ff = expert_gate.shape[1:]
    capacity = 4 * tok // sp_n
    y_n = tp_n // 2
    groups, rows = sp_n // PAIR, PAIR * capacity
    wide = -(-tok // 128) * 128
    vmem = pl.BlockSpec(memory_space=pltpu.VMEM)
    hbm = pl.BlockSpec(memory_space=pl.ANY)
    dma = pltpu.SemaphoreType.DMA
    scratch = [
        pltpu.VMEM((chan, width), BF16),
        pltpu.VMEM((tok, feat), BF16),
        pltpu.VMEM((width, ff), BF16),
        pltpu.VMEM((width, ff), BF16),
        pltpu.VMEM((ff, width), BF16),
        pltpu.VMEM((HALO, chan), BF16),
        pltpu.VMEM((HALO, chan), BF16),
        pltpu.VMEM((HALO, 128), jnp.int32),
        pltpu.VMEM((8, wide), F32),
        pltpu.VMEM((tok, 128), F32),
        pltpu.VMEM((HALO + tok, chan), F32),
        pltpu.VMEM((HALO + tok, 128), jnp.int32),
        pltpu.VMEM((tok, chan), F32),
        pltpu.VMEM((3, 8, wide), F32),
        pltpu.VMEM((3, tp_n, 8, wide), F32),
        pltpu.VMEM((y_n, tok, feat), BF16),
        pltpu.VMEM((y_n, tok, feat), BF16),
        pltpu.VMEM((y_n, tok, feat), BF16),
        pltpu.VMEM((y_n, tok, feat), BF16),
        pltpu.VMEM((tok, feat), BF16),
        pltpu.VMEM((sp_n, capacity, feat), BF16),
        pltpu.VMEM((tp_n, sp_n, capacity, feat), BF16),
        pltpu.VMEM((groups, rows, ff), BF16),
        pltpu.VMEM((groups, y_n, rows, feat), BF16),
        pltpu.VMEM((groups, y_n, rows, feat), BF16),
        pltpu.VMEM((groups, y_n, rows, feat), BF16),
        pltpu.VMEM((groups, y_n, rows, feat), BF16),
        pltpu.VMEM((groups, y_n, rows, feat), F32),
        pltpu.VMEM((sp_n, capacity, feat), BF16),
        pltpu.VMEM((sp_n, capacity, feat), BF16),
        dma((5,)),
        dma((2, 2)),
        dma((3, tp_n)),
        dma((3, tp_n)),
        dma((2, y_n)),
        dma((2, y_n)),
        dma((sp_n,)),
        dma((sp_n,)),
        dma((2 * y_n - 1, sp_n)),
        dma((2 * y_n - 1, sp_n)),
        dma((groups, y_n)),
        dma((groups, y_n)),
        dma((groups, y_n, PAIR)),
        dma((groups, y_n, PAIR)),
        dma((sp_n,)),
        dma((sp_n,)),
    ]
    return pl.pallas_call(
        functools.partial(block_kernel, sp_n, tp_n, capacity, conv_kernel.shape[0]),
        out_shape=jax.ShapeDtypeStruct((tok, feat), BF16),
        in_specs=[vmem] * 5 + [hbm] * 2 + [vmem] * 3 + [hbm] * 3 + [vmem],
        out_specs=vmem,
        scratch_shapes=scratch,
        compiler_params=pltpu.CompilerParams(
            collective_id=0, has_side_effects=True, vmem_limit_bytes=60 * 1024 * 1024
        ),
    )(
        glu_value,
        glu_gate,
        doc_ids[None, :],
        conv_kernel,
        conv_gain[None, :],
        out_weight,
        residual,
        mix_gain[None, :],
        routes.T,
        route_weights.T,
        expert_gate,
        expert_up,
        expert_down,
        final_gain[None, :],
    )


def local(*args):
    sp_n, tp_n = lax.axis_size("sp"), lax.axis_size("tp")
    tok, chan = args[0].shape
    ff = args[10].shape[2]
    feat = args[13].shape[0]
    aligned = (
        chan % 128 == 0
        and feat % TILE == 0
        and ff % TILE == 0
        and (4 * tok // sp_n) % 32 == 0
        and tok % HALO == 0
        and args[3].shape[0] <= HALO
        and tp_n % 2 == 0
        and tp_n > 2
        and sp_n & (sp_n - 1) == 0
        and sp_n > 2 * PAIR
        and sp_n <= 128
        and args[10].shape[0] == 1
    )
    return (local_kernel if aligned else local_plain)(*args)


def solution(mesh):
    return jax.shard_map(
        local,
        mesh=mesh,
        in_specs=(
            P("sp", "tp"),
            P("sp", "tp"),
            P("sp"),
            P(None, "tp"),
            P("tp"),
            P("tp", None),
            P("sp", None),
            P(),
            P("sp", None),
            P("sp", None),
            P("sp", None, "tp"),
            P("sp", None, "tp"),
            P("sp", "tp", None),
            P("tp"),
        ),
        out_specs=P("sp", "tp"),
        check_vma=False,
    )
```

```python
import functools

import jax
import jax.numpy as jnp
from jax import lax
from jax.experimental import pallas as pl
from jax.experimental.pallas import tpu as pltpu
from jax.sharding import PartitionSpec as P

residual_alpha = 1.41421356
norm_eps = 1e-05


def from_behind(value, axis, by):
    peers = lax.axis_size(axis)
    pairs = [(i, i + by) for i in range(peers) if 0 <= i + by < peers]
    return lax.ppermute(value, axis, pairs)


def scaled_norm(pre_norm, gain):
    row_mean = jnp.mean(pre_norm, -1, keepdims=True)
    row_var = jnp.mean(pre_norm * pre_norm, -1, keepdims=True) - row_mean * row_mean
    return (pre_norm - row_mean) * lax.rsqrt(row_var + norm_eps) * gain


def local_plain(
    glu_value,
    glu_gate,
    doc_ids,
    conv_kernel,
    conv_gain,
    out_weight,
    residual,
    mix_gain,
    routes,
    route_weights,
    expert_gate,
    expert_up,
    expert_down,
    final_gain,
):
    tok_rows = glu_value.shape[0]
    rim_len = conv_kernel.shape[0] - 1
    channels = glu_value.shape[1] * lax.axis_size("tp")
    gated_rows = (
        glu_value.astype(jnp.float32) * jax.nn.sigmoid(glu_gate.astype(jnp.float32))
    ).astype(jnp.bfloat16)
    rim_rows, rim_ids = from_behind(
        (gated_rows[tok_rows - rim_len :], doc_ids[tok_rows - rim_len :]), "sp", 1
    )
    extended = jnp.concatenate([rim_rows, gated_rows], 0).astype(jnp.float32)
    ext_ids = jnp.concatenate([rim_ids, doc_ids], 0)
    kernel = conv_kernel.astype(jnp.float32)
    filtered = jnp.zeros(gated_rows.shape, jnp.float32)
    for shift_by in range(rim_len + 1):
        begin_at = rim_len - shift_by
        same_doc = (ext_ids[begin_at : begin_at + tok_rows] == doc_ids)[:, None]
        filtered = (
            filtered
            + jnp.where(same_doc, extended[begin_at : begin_at + tok_rows], 0.0) * kernel[shift_by]
        )
    row_sum, row_square = lax.psum((jnp.sum(filtered, 1), jnp.sum(filtered * filtered, 1)), "tp")
    row_mean = row_sum[:, None] / channels
    row_var = row_square[:, None] / channels - row_mean * row_mean
    conv_out = jax.nn.silu(
        (filtered - row_mean) * lax.rsqrt(row_var + norm_eps) * conv_gain
    ).astype(jnp.bfloat16)
    mix_total = lax.psum(
        jnp.dot(conv_out, out_weight, preferred_element_type=jnp.float32).astype(jnp.bfloat16), "tp"
    ).astype(jnp.float32)
    mixed_rows = scaled_norm(
        residual_alpha * residual.astype(jnp.float32) + mix_total, mix_gain
    ).astype(jnp.bfloat16)
    experts = expert_gate.shape[0] * lax.axis_size("sp")
    capacity = 4 * tok_rows // experts
    chosen = routes.reshape(-1)
    member = (chosen[:, None] == jnp.arange(experts, dtype=jnp.int32)[None, :]).astype(jnp.int32)
    earlier = jnp.cumsum(member, 0) - member
    slot_index = chosen * capacity + jnp.sum(earlier * member, 1)
    dispatch_table = jnp.any(
        jnp.arange(experts * capacity, dtype=jnp.int32)[:, None, None]
        == slot_index.reshape(tok_rows, 2)[None],
        -1,
    ).astype(jnp.bfloat16)
    feat_block = mixed_rows.shape[1] // lax.axis_size("tp")
    offset = lax.axis_index("tp") * feat_block
    w_gate = expert_gate[0]
    w_up = expert_up[0]
    w_down = expert_down[0]
    row_slice = lax.dynamic_slice_in_dim(mixed_rows, offset, feat_block, 1)
    outgoing = (
        jnp.dot(dispatch_table, row_slice, preferred_element_type=jnp.float32)
        .astype(jnp.bfloat16)
        .reshape(experts, capacity, feat_block)
    )
    arrived = lax.all_to_all(outgoing, "sp", split_axis=0, concat_axis=0, tiled=True)
    sources, slot_count, part_width = arrived.shape
    flat_rows = arrived.reshape(sources * slot_count, part_width)
    col_piece = lax.all_gather(flat_rows, "tp", axis=1, tiled=True)
    gate_proj = jnp.dot(col_piece, w_gate, preferred_element_type=jnp.float32)
    up_proj = jnp.dot(col_piece, w_up, preferred_element_type=jnp.float32)
    hidden = (jax.nn.silu(gate_proj) * up_proj).astype(jnp.bfloat16)
    partial_value = jnp.dot(hidden, w_down, preferred_element_type=jnp.float32).reshape(
        sources, slot_count, -1
    )
    summed = lax.psum_scatter(
        partial_value.astype(jnp.bfloat16), "tp", scatter_dimension=2, tiled=True
    )
    returned = lax.all_to_all(summed, "sp", split_axis=0, concat_axis=0, tiled=True)
    flat_back = returned.reshape(experts * capacity, feat_block)
    picked = flat_back[slot_index].astype(jnp.float32).reshape(tok_rows, 2, feat_block)
    moe_sum = jnp.sum(route_weights[:, :, None] * picked, 1)
    own_cols = lax.dynamic_slice_in_dim(mixed_rows, offset, feat_block, 1).astype(jnp.float32)
    pre_norm = residual_alpha * own_cols + moe_sum
    fin_sum, fin_square = lax.psum((jnp.sum(pre_norm, 1), jnp.sum(pre_norm * pre_norm, 1)), "tp")
    features = feat_block * lax.axis_size("tp")
    fin_mean = fin_sum[:, None] / features
    fin_var = fin_square[:, None] / features - fin_mean * fin_mean
    return ((pre_norm - fin_mean) * lax.rsqrt(fin_var + norm_eps) * final_gain).astype(jnp.bfloat16)


HALO = 32
PAIR = 2
TILE = 256
TURNS = (0, 4, 1, 6, 2, 5, 7, 3)
PLAN = (
    ("D0", "D1", "D2", "D4", "F0", "D3", "D7", "L2", "D5", "D6", "L4", "L1", "F2", "F1",),
    (("L3",), ("F4", "L7",), (), ("F3", "L5",)),
    (("X0",), ("F7", "L6",), (), ("F5",)),
    (("X1",), (), ("R0", "R1",), ("F6",)),
    (("X2",), (), ("R3", "R2",), ()),
    ("X3", "R5", "R4", "R6", "R7",),
)
F32 = jnp.float32
BF16 = jnp.bfloat16


def block_kernel(
    sp_n,
    tp_n,
    capacity,
    taps,
    glu_value_hbm,
    glu_gate_hbm,
    ids_hbm,
    conv_kernel_hbm,
    conv_gain_hbm,
    out_weight_hbm,
    residual_hbm,
    mix_gain_hbm,
    routes_hbm,
    weights_hbm,
    gate_hbm,
    up_hbm,
    down_hbm,
    final_gain_hbm,
    out,
    glu_value,
    glu_gate,
    ids_row,
    conv_kernel,
    conv_gain,
    mix_gain,
    routes_row,
    weights_row,
    final_gain,
    w_out,
    resid,
    w_gate,
    w_up,
    w_down,
    rim_out,
    rim_in,
    rim_ids,
    by_row,
    by_col,
    ext,
    ext_ids,
    fil,
    stat_out,
    stat_in,
    mix_pp,
    mix_a,
    mix_s,
    mix_b,
    mixed,
    outbox,
    rows_in,
    hidden,
    part_pp,
    part_a,
    part_s,
    part_b,
    part_own,
    back_out,
    back_in,
    small_sem,
    load_sem,
    halo_sem,
    stat_send,
    stat_recv,
    mix_send,
    mix_recv,
    disp_send,
    disp_recv,
    ag_send,
    ag_recv,
    part_send,
    part_recv,
    cross_send,
    cross_recv,
    back_send,
    back_recv,
):
    tok, chan = glu_value.shape
    feat = final_gain_hbm.shape[1]
    ff = hidden.shape[2]
    y_n = tp_n // 2
    sp = lax.axis_index("sp")
    tp = lax.axis_index("tp")
    y = tp // 2
    core = tp % 2
    partner = y * 2 + (1 - core)
    groups = sp_n // PAIR
    group_rows = PAIR * capacity
    pending = []

    def y_at(k):
        return lax.rem(y + k, y_n)

    def peer(p):
        to, bit = sp, 1
        while bit < sp_n:
            if TURNS[p] & bit:
                to = to + bit - 2 * bit * lax.rem(lax.div(sp, bit), 2)
            bit *= 2
        return to

    def feat_cols(block):
        return pl.ds(pl.multiple_of(block * feat, feat), feat)

    def remote(src, dst, send, recv, axis, to):
        return pltpu.make_async_remote_copy(
            src_ref=src,
            dst_ref=dst,
            send_sem=send,
            recv_sem=recv,
            device_id={axis: to},
            device_id_type=pl.DeviceIdType.MESH,
        )

    def send(*args):
        copy = remote(*args)
        copy.start()
        pending.append(copy)

    def arrived(dst, recv, send_sem, axis, to):
        remote(dst, dst, send_sem, recv, axis, to).wait_recv()

    barrier = pltpu.get_barrier_semaphore()
    for k in range(1, sp_n):
        pl.semaphore_signal(
            barrier, inc=1, device_id={"sp": lax.rem(sp + k, sp_n)},
            device_id_type=pl.DeviceIdType.MESH,
        )
    for k in range(1, tp_n):
        pl.semaphore_signal(
            barrier, inc=1, device_id={"tp": lax.rem(tp + k, tp_n)},
            device_id_type=pl.DeviceIdType.MESH,
        )

    smalls = []
    for i, (src, dst) in enumerate(
        (
            (ids_hbm, ids_row),
            (routes_hbm, routes_row),
            (weights_hbm, weights_row),
            (glu_value_hbm, glu_value),
            (glu_gate_hbm, glu_gate),
            (conv_kernel_hbm, conv_kernel),
            (conv_gain_hbm, conv_gain),
            (mix_gain_hbm, mix_gain),
            (final_gain_hbm, final_gain),
        )
    ):
        copy = pltpu.make_async_copy(src, dst, small_sem.at[i])
        copy.start()
        smalls.append(copy)
    for copy in smalls:
        copy.wait()
    loads = []
    for i, (src, dst) in enumerate(
        (
            (out_weight_hbm, w_out),
            (residual_hbm.at[:, feat_cols(tp)], resid),
            (gate_hbm.at[0], w_gate),
            (up_hbm.at[0], w_up),
            (down_hbm.at[0], w_down),
        )
    ):
        copy = pltpu.make_async_copy(src, dst, load_sem.at[i])
        copy.start()
        loads.append(copy)

    lanes = 128
    wide = by_row.shape[1]
    by_row[...] = jnp.zeros_like(by_row)
    by_row[0:1, 0:tok] = ids_row[...].astype(F32)
    by_row[1:3, 0:tok] = routes_row[...].astype(F32)
    by_row[3:5, 0:tok] = weights_row[...]
    by_col[...] = jnp.concatenate([by_row[...], jnp.zeros((lanes - 8, wide), F32)], 0).T[:tok]
    ext_ids[HALO:, :] = jnp.broadcast_to(by_col[:, 0:1].astype(jnp.int32), (tok, lanes))

    value = glu_value[...].astype(F32)
    gated = (value * jax.nn.sigmoid(glu_gate[...].astype(F32))).astype(BF16)
    ext[HALO:, :] = gated.astype(F32)
    rim_out[...] = gated[tok - HALO :]

    lower = (
        lax.broadcasted_iota(jnp.int32, (tok, tok), 1)
        < lax.broadcasted_iota(jnp.int32, (tok, tok), 0)
    )
    upper = (
        lax.broadcasted_iota(jnp.int32, (tok, tok), 0)
        < lax.broadcasted_iota(jnp.int32, (tok, tok), 1)
    )
    e_lane = lax.broadcasted_iota(jnp.int32, (tok, lanes), 1)
    one_lane = lax.broadcasted_iota(jnp.int32, (1, lanes), 1)
    subs = -(-sp_n // 16) * 16
    e_sub = lax.broadcasted_iota(jnp.int32, (subs, tok), 0)
    lane_expert = jnp.full((1, lanes), -1, jnp.int32)
    sub_expert = jnp.full((subs, tok), -1, jnp.int32)
    for r in range(sp_n):
        lane_expert = jnp.where(one_lane == r, peer(r), lane_expert)
        sub_expert = jnp.where(e_sub == r, peer(r), sub_expert)
    lane_expert = lane_expert.astype(F32)
    m0 = (by_col[:, 1:2] == lane_expert).astype(F32)
    m1 = (by_col[:, 2:3] == lane_expert).astype(F32)
    rank = jnp.dot(lower.astype(F32).astype(BF16), (m0 + m1).astype(BF16), preferred_element_type=F32)
    place = rank + (e_lane * capacity).astype(F32)
    slot_col0 = jnp.sum(m0 * place, 1, keepdims=True).astype(jnp.int32)
    slot_col1 = jnp.sum(m1 * place, 1, keepdims=True).astype(jnp.int32)
    n0 = (routes_row[0:1, :] == sub_expert).astype(F32)
    n1 = (routes_row[1:2, :] == sub_expert).astype(F32)
    rank_r = jnp.dot((n0 + n1).astype(BF16), upper.astype(F32).astype(BF16), preferred_element_type=F32)
    place_r = rank_r + (e_sub * capacity).astype(F32)
    slot_row0 = jnp.sum(n0 * place_r, 0, keepdims=True).astype(jnp.int32)
    slot_row1 = jnp.sum(n1 * place_r, 0, keepdims=True).astype(jnp.int32)

    pl.semaphore_wait(barrier, sp_n + tp_n - 2)

    right = lax.rem(sp + 1, sp_n)
    halo = [
        remote(src, dst, halo_sem.at[0, i], halo_sem.at[1, i], "sp", right)
        for i, (src, dst) in enumerate(
            ((rim_out, rim_in), (ext_ids.at[pl.ds(tok, HALO)], rim_ids))
        )
    ]

    @pl.when(sp < sp_n - 1)
    def _():
        for copy in halo:
            copy.start()

    kern = conv_kernel[...].astype(F32)
    lane_blocks = chan // lanes

    def convolve(at):
        own = ext_ids[HALO + at : 2 * HALO + at, :]
        acc = [jnp.zeros((HALO, lanes), F32) for _ in range(lane_blocks)]
        for lag in range(taps):
            begin = HALO + at - lag
            same = ext_ids[begin : begin + HALO, :] == own
            for b in range(lane_blocks):
                part = ext[begin : begin + HALO, b * lanes : (b + 1) * lanes]
                acc[b] = acc[b] + jnp.where(same, part, 0.0) * kern[lag : lag + 1, b * lanes : (b + 1) * lanes]
        for b in range(lane_blocks):
            fil[at : at + HALO, b * lanes : (b + 1) * lanes] = acc[b]

    for at in range(HALO, tok, HALO):
        convolve(at)

    @pl.when(sp == 0)
    def _():
        ext[:HALO, :] = jnp.zeros((HALO, chan), F32)
        ext_ids[:HALO, :] = jnp.full((HALO, lanes), -1, jnp.int32)

    @pl.when(sp > 0)
    def _():
        for copy in halo:
            copy.wait_recv()
        ext[:HALO, :] = rim_in[...].astype(F32)
        ext_ids[:HALO, :] = rim_ids[...]

    convolve(0)

    def stats(i, value, width):
        row_sum = jnp.sum(value, 1, keepdims=True)
        row_square = jnp.sum(value * value, 1, keepdims=True)
        packed = jnp.where(e_lane == 0, row_sum, jnp.where(e_lane == 1, row_square, 0.0))
        packed = jnp.concatenate([packed, jnp.zeros((wide - tok, lanes), F32)], 0)
        stat_out[i] = packed.T[:8]
        for k in range(1, tp_n):
            send(
                stat_out.at[i], stat_in.at[i, k], stat_send.at[i, k], stat_recv.at[i, k],
                "tp", lax.rem(tp + k, tp_n),
            )
        total = stat_out[i]
        for k in range(1, tp_n):
            arrived(stat_in.at[i, k], stat_recv.at[i, k], stat_send.at[i, k], "tp", partner)
            total = total + stat_in[i, k]
        total = jnp.concatenate([total, jnp.zeros((lanes - 8, wide), F32)], 0).T[:tok]
        mean = total[:, 0:1] / width
        var = total[:, 1:2] / width - mean * mean
        return mean, lax.rsqrt(var + norm_eps)

    filtered = fil[...]
    mean, scale = stats(0, filtered, chan * tp_n)
    normed = (filtered - mean) * scale * conv_gain[...]
    conv_out = (normed * jax.nn.sigmoid(normed)).astype(BF16)

    loads[0].wait()
    order = list(range(1, y_n)) + [0]
    for k in order:
        cols = feat_cols(2 * y_at(k) + 1 - core)
        mix_pp[k] = jnp.dot(conv_out, w_out[:, cols], preferred_element_type=F32).astype(BF16)
        send(mix_pp.at[k], mix_a.at[k], mix_send.at[0, k], mix_recv.at[0, k], "tp", partner)
    own_mix = None
    for k in order:
        cols = feat_cols(2 * y_at(k) + core)
        value = jnp.dot(conv_out, w_out[:, cols], preferred_element_type=F32)
        arrived(mix_a.at[k], mix_recv.at[0, k], mix_send.at[0, k], "tp", partner)
        value = value + mix_a[k].astype(F32)
        if k:
            mix_s[k] = value.astype(BF16)
            send(
                mix_s.at[k], mix_b.at[k], mix_send.at[1, k], mix_recv.at[1, k],
                "tp", 2 * y_at(k) + core,
            )
        else:
            own_mix = value
    loads[1].wait()
    pre = own_mix + residual_alpha * resid[...].astype(F32)
    for k in range(1, y_n):
        arrived(mix_b.at[k], mix_recv.at[1, k], mix_send.at[1, k], "tp", partner)
        pre = pre + mix_b[k].astype(F32)
    mean, scale = stats(1, pre, feat * tp_n)
    mixed[...] = ((pre - mean) * scale * mix_gain[:, feat_cols(tp)]).astype(BF16)

    def spread(d):
        block = rows_in.at[tp, d]
        send(block, block, ag_send.at[0, d], ag_recv.at[0, d], "tp", partner)
        for k in range(1, y_n):
            send(
                block, block, ag_send.at[k, d], ag_recv.at[k, d],
                "tp", 2 * y_at(k) + core,
            )

    def pass_on(d):
        for k in range(1, y_n):
            block = rows_in.at[2 * y_at(y_n - k) + core, d]
            arrived(block, ag_recv.at[k, d], ag_send.at[k, d], "tp", partner)
            send(
                block, block, ag_send.at[y_n - 1 + k, d], ag_recv.at[y_n - 1 + k, d],
                "tp", partner,
            )

    def gathered(d):
        block = rows_in.at[partner, d]
        arrived(block, ag_recv.at[0, d], ag_send.at[0, d], "tp", partner)
        for k in range(1, y_n):
            block = rows_in.at[2 * y_at(y_n - k) + 1 - core, d]
            arrived(block, ag_recv.at[y_n - 1 + k, d], ag_send.at[y_n - 1 + k, d], "tp", partner)

    def dispatch(p):
        s_at = lax.broadcasted_iota(jnp.int32, (capacity, tok), 0) + p * capacity
        table = jnp.logical_or(s_at == slot_row0, s_at == slot_row1).astype(F32).astype(BF16)
        block = jnp.dot(table, mixed[...], preferred_element_type=F32).astype(BF16)
        if p:
            outbox[p] = block
            send(
                outbox.at[p], rows_in.at[tp, p], disp_send.at[p], disp_recv.at[p],
                "sp", peer(p),
            )
        else:
            rows_in[tp, 0] = block
            spread(0)

    def landed(p):
        arrived(rows_in.at[tp, p], disp_recv.at[p], disp_send.at[p], "sp", right)
        spread(p)

    def gate_up(g, n):
        cols = pl.ds(n * TILE, TILE)
        rows = [
            rows_in[j, PAIR * g : PAIR * (g + 1)].reshape(group_rows, feat) for j in range(tp_n)
        ]
        x = jnp.concatenate(rows, 1)
        gate = jnp.dot(x, w_gate[:, cols], preferred_element_type=F32)
        up = jnp.dot(x, w_up[:, cols], preferred_element_type=F32)
        hidden[g, :, cols] = (gate * jax.nn.sigmoid(gate) * up).astype(BF16)

    def down(g):
        def part(block):
            return jnp.dot(hidden[g], w_down[:, feat_cols(block)], preferred_element_type=F32)

        for k in order:
            part_pp[g, k] = part(2 * y_at(k) + 1 - core).astype(BF16)
            send(
                part_pp.at[g, k], part_a.at[g, k], part_send.at[g, k], part_recv.at[g, k],
                "tp", partner,
            )
            part_own[g, k] = part(2 * y_at(k) + core)

    def cross(g):
        for k in order[:-1]:
            arrived(part_a.at[g, k], part_recv.at[g, k], part_send.at[g, k], "tp", partner)
            part_s[g, k] = (part_own[g, k] + part_a[g, k].astype(F32)).astype(BF16)
            for i in ((0, 1) if g == groups - 1 else (1, 0)):
                rows = pl.ds(i * capacity, capacity)
                send(
                    part_s.at[g, k, rows], part_b.at[g, k, rows],
                    cross_send.at[g, k, i], cross_recv.at[g, k, i],
                    "tp", 2 * y_at(k) + core,
                )
        arrived(part_a.at[g, 0], part_recv.at[g, 0], part_send.at[g, 0], "tp", partner)

    def finish(p):
        g, i = p // PAIR, p % PAIR
        rows = pl.ds(i * capacity, capacity)
        value = part_own[g, 0, rows, :] + part_a[g, 0, rows, :].astype(F32)
        for k in range(1, y_n):
            arrived(
                part_b.at[g, k, rows], cross_recv.at[g, k, i], cross_send.at[g, k, i],
                "tp", partner,
            )
            value = value + part_b[g, k, rows, :].astype(F32)
        if p:
            back_out[p] = value.astype(BF16)
            send(
                back_out.at[p], back_in.at[p], back_send.at[p], back_recv.at[p],
                "sp", peer(p),
            )
        else:
            back_in[0] = value.astype(BF16)

    tiles = ff // TILE
    early = PLAN[0]
    do = dict(D=dispatch, L=landed, F=pass_on, R=finish, X=cross)

    def act(text):
        for word in text:
            do[word[0]](int(word[1:]))

    act(early)
    loads[2].wait()
    loads[3].wait()
    for g in range(groups):
        for p in range(PAIR * g, PAIR * (g + 1)):
            gathered(p)
        for n in range(tiles):
            gate_up(g, n)
            if n % 2 or n == tiles - 1:
                act(PLAN[1 + g][n // 2])
        if g == 0:
            loads[4].wait()
        down(g)
        act(PLAN[1 + g][3])
    act(PLAN[-1])

    def combine(lo, hi):
        for p in range(max(lo, 1), hi):
            arrived(back_in.at[p], back_recv.at[p], back_send.at[p], "sp", right)
        slots = (hi - lo) * capacity
        rows = back_in[lo:hi].reshape(slots, feat)
        s_lane = lax.broadcasted_iota(jnp.int32, (tok, slots), 1) + lo * capacity
        pick0 = jnp.dot((s_lane == slot_col0).astype(F32).astype(BF16), rows, preferred_element_type=F32)
        pick1 = jnp.dot((s_lane == slot_col1).astype(F32).astype(BF16), rows, preferred_element_type=F32)
        return by_col[:, 3:4] * pick0 + by_col[:, 4:5] * pick1

    moe = combine(0, sp_n - PAIR) + combine(sp_n - PAIR, sp_n)
    pre = residual_alpha * mixed[...].astype(F32) + moe
    mean, scale = stats(2, pre, feat * tp_n)
    out[...] = ((pre - mean) * scale * final_gain[...]).astype(BF16)
    for copy in pending:
        copy.wait_send()

    @pl.when(sp < sp_n - 1)
    def _():
        for copy in halo:
            copy.wait_send()


def local_kernel(
    glu_value,
    glu_gate,
    doc_ids,
    conv_kernel,
    conv_gain,
    out_weight,
    residual,
    mix_gain,
    routes,
    route_weights,
    expert_gate,
    expert_up,
    expert_down,
    final_gain,
):
    sp_n, tp_n = lax.axis_size("sp"), lax.axis_size("tp")
    tok, chan = glu_value.shape
    feat = final_gain.shape[0]
    width, ff = expert_gate.shape[1:]
    capacity = 4 * tok // sp_n
    y_n = tp_n // 2
    groups, rows = sp_n // PAIR, PAIR * capacity
    wide = -(-tok // 128) * 128
    vmem = pl.BlockSpec(memory_space=pltpu.VMEM)
    hbm = pl.BlockSpec(memory_space=pl.ANY)
    dma = pltpu.SemaphoreType.DMA
    scratch = [
        pltpu.VMEM((tok, chan), BF16),
        pltpu.VMEM((tok, chan), BF16),
        pltpu.VMEM((1, tok), jnp.int32),
        pltpu.VMEM(conv_kernel.shape, BF16),
        pltpu.VMEM((1, chan), F32),
        pltpu.VMEM((1, width), F32),
        pltpu.VMEM((2, tok), jnp.int32),
        pltpu.VMEM((2, tok), F32),
        pltpu.VMEM((1, feat), F32),
        pltpu.VMEM((chan, width), BF16),
        pltpu.VMEM((tok, feat), BF16),
        pltpu.VMEM((width, ff), BF16),
        pltpu.VMEM((width, ff), BF16),
        pltpu.VMEM((ff, width), BF16),
        pltpu.VMEM((HALO, chan), BF16),
        pltpu.VMEM((HALO, chan), BF16),
        pltpu.VMEM((HALO, 128), jnp.int32),
        pltpu.VMEM((8, wide), F32),
        pltpu.VMEM((tok, 128), F32),
        pltpu.VMEM((HALO + tok, chan), F32),
        pltpu.VMEM((HALO + tok, 128), jnp.int32),
        pltpu.VMEM((tok, chan), F32),
        pltpu.VMEM((3, 8, wide), F32),
        pltpu.VMEM((3, tp_n, 8, wide), F32),
        pltpu.VMEM((y_n, tok, feat), BF16),
        pltpu.VMEM((y_n, tok, feat), BF16),
        pltpu.VMEM((y_n, tok, feat), BF16),
        pltpu.VMEM((y_n, tok, feat), BF16),
        pltpu.VMEM((tok, feat), BF16),
        pltpu.VMEM((sp_n, capacity, feat), BF16),
        pltpu.VMEM((tp_n, sp_n, capacity, feat), BF16),
        pltpu.VMEM((groups, rows, ff), BF16),
        pltpu.VMEM((groups, y_n, rows, feat), BF16),
        pltpu.VMEM((groups, y_n, rows, feat), BF16),
        pltpu.VMEM((groups, y_n, rows, feat), BF16),
        pltpu.VMEM((groups, y_n, rows, feat), BF16),
        pltpu.VMEM((groups, y_n, rows, feat), F32),
        pltpu.VMEM((sp_n, capacity, feat), BF16),
        pltpu.VMEM((sp_n, capacity, feat), BF16),
        dma((9,)),
        dma((5,)),
        dma((2, 2)),
        dma((3, tp_n)),
        dma((3, tp_n)),
        dma((2, y_n)),
        dma((2, y_n)),
        dma((sp_n,)),
        dma((sp_n,)),
        dma((2 * y_n - 1, sp_n)),
        dma((2 * y_n - 1, sp_n)),
        dma((groups, y_n)),
        dma((groups, y_n)),
        dma((groups, y_n, PAIR)),
        dma((groups, y_n, PAIR)),
        dma((sp_n,)),
        dma((sp_n,)),
    ]
    return pl.pallas_call(
        functools.partial(block_kernel, sp_n, tp_n, capacity, conv_kernel.shape[0]),
        out_shape=pltpu.VMEM((tok, feat), BF16),
        in_specs=[hbm] * 14,
        out_specs=vmem,
        scratch_shapes=scratch,
        compiler_params=pltpu.CompilerParams(
            collective_id=0, has_side_effects=True, vmem_limit_bytes=60 * 1024 * 1024
        ),
    )(
        glu_value,
        glu_gate,
        doc_ids[None, :],
        conv_kernel,
        conv_gain[None, :],
        out_weight,
        residual,
        mix_gain[None, :],
        routes.T,
        route_weights.T,
        expert_gate,
        expert_up,
        expert_down,
        final_gain[None, :],
    )


def local(*args):
    sp_n, tp_n = lax.axis_size("sp"), lax.axis_size("tp")
    tok, chan = args[0].shape
    ff = args[10].shape[2]
    feat = args[13].shape[0]
    aligned = (
        chan % 128 == 0
        and feat % TILE == 0
        and ff % TILE == 0
        and (4 * tok // sp_n) % 32 == 0
        and tok % HALO == 0
        and args[3].shape[0] <= HALO
        and tp_n % 2 == 0
        and tp_n > 2
        and sp_n == len(TURNS)
        and -(-ff // (2 * TILE)) <= len(PLAN[1]) - 1
        and args[10].shape[0] == 1
    )
    return (local_kernel if aligned else local_plain)(*args)


def solution(mesh):
    return jax.shard_map(
        local,
        mesh=mesh,
        in_specs=(
            P("sp", "tp"),
            P("sp", "tp"),
            P("sp"),
            P(None, "tp"),
            P("tp"),
            P("tp", None),
            P("sp", None),
            P(),
            P("sp", None),
            P("sp", None),
            P("sp", None, "tp"),
            P("sp", None, "tp"),
            P("sp", "tp", None),
            P("tp"),
        ),
        out_specs=P("sp", "tp"),
        check_vma=False,
    )
```

```python
import functools

import jax
import jax.numpy as jnp
from jax import lax
from jax.experimental import pallas as pl
from jax.experimental.pallas import tpu as pltpu
from jax.sharding import PartitionSpec as P

residual_alpha = 1.41421356
norm_eps = 1e-05


def from_behind(value, axis, by):
    peers = lax.axis_size(axis)
    pairs = [(i, i + by) for i in range(peers) if 0 <= i + by < peers]
    return lax.ppermute(value, axis, pairs)


def scaled_norm(pre_norm, gain):
    row_mean = jnp.mean(pre_norm, -1, keepdims=True)
    row_var = jnp.mean(pre_norm * pre_norm, -1, keepdims=True) - row_mean * row_mean
    return (pre_norm - row_mean) * lax.rsqrt(row_var + norm_eps) * gain


def local_plain(
    glu_value,
    glu_gate,
    doc_ids,
    conv_kernel,
    conv_gain,
    out_weight,
    residual,
    mix_gain,
    routes,
    route_weights,
    expert_gate,
    expert_up,
    expert_down,
    final_gain,
):
    tok_rows = glu_value.shape[0]
    rim_len = conv_kernel.shape[0] - 1
    channels = glu_value.shape[1] * lax.axis_size("tp")
    gated_rows = (
        glu_value.astype(jnp.float32) * jax.nn.sigmoid(glu_gate.astype(jnp.float32))
    ).astype(jnp.bfloat16)
    rim_rows, rim_ids = from_behind(
        (gated_rows[tok_rows - rim_len :], doc_ids[tok_rows - rim_len :]), "sp", 1
    )
    extended = jnp.concatenate([rim_rows, gated_rows], 0).astype(jnp.float32)
    ext_ids = jnp.concatenate([rim_ids, doc_ids], 0)
    kernel = conv_kernel.astype(jnp.float32)
    filtered = jnp.zeros(gated_rows.shape, jnp.float32)
    for shift_by in range(rim_len + 1):
        begin_at = rim_len - shift_by
        same_doc = (ext_ids[begin_at : begin_at + tok_rows] == doc_ids)[:, None]
        filtered = (
            filtered
            + jnp.where(same_doc, extended[begin_at : begin_at + tok_rows], 0.0) * kernel[shift_by]
        )
    row_sum, row_square = lax.psum((jnp.sum(filtered, 1), jnp.sum(filtered * filtered, 1)), "tp")
    row_mean = row_sum[:, None] / channels
    row_var = row_square[:, None] / channels - row_mean * row_mean
    conv_out = jax.nn.silu(
        (filtered - row_mean) * lax.rsqrt(row_var + norm_eps) * conv_gain
    ).astype(jnp.bfloat16)
    mix_total = lax.psum(
        jnp.dot(conv_out, out_weight, preferred_element_type=jnp.float32).astype(jnp.bfloat16), "tp"
    ).astype(jnp.float32)
    mixed_rows = scaled_norm(
        residual_alpha * residual.astype(jnp.float32) + mix_total, mix_gain
    ).astype(jnp.bfloat16)
    experts = expert_gate.shape[0] * lax.axis_size("sp")
    capacity = 4 * tok_rows // experts
    chosen = routes.reshape(-1)
    member = (chosen[:, None] == jnp.arange(experts, dtype=jnp.int32)[None, :]).astype(jnp.int32)
    earlier = jnp.cumsum(member, 0) - member
    slot_index = chosen * capacity + jnp.sum(earlier * member, 1)
    dispatch_table = jnp.any(
        jnp.arange(experts * capacity, dtype=jnp.int32)[:, None, None]
        == slot_index.reshape(tok_rows, 2)[None],
        -1,
    ).astype(jnp.bfloat16)
    feat_block = mixed_rows.shape[1] // lax.axis_size("tp")
    offset = lax.axis_index("tp") * feat_block
    w_gate = expert_gate[0]
    w_up = expert_up[0]
    w_down = expert_down[0]
    row_slice = lax.dynamic_slice_in_dim(mixed_rows, offset, feat_block, 1)
    outgoing = (
        jnp.dot(dispatch_table, row_slice, preferred_element_type=jnp.float32)
        .astype(jnp.bfloat16)
        .reshape(experts, capacity, feat_block)
    )
    arrived = lax.all_to_all(outgoing, "sp", split_axis=0, concat_axis=0, tiled=True)
    sources, slot_count, part_width = arrived.shape
    flat_rows = arrived.reshape(sources * slot_count, part_width)
    col_piece = lax.all_gather(flat_rows, "tp", axis=1, tiled=True)
    gate_proj = jnp.dot(col_piece, w_gate, preferred_element_type=jnp.float32)
    up_proj = jnp.dot(col_piece, w_up, preferred_element_type=jnp.float32)
    hidden = (jax.nn.silu(gate_proj) * up_proj).astype(jnp.bfloat16)
    partial_value = jnp.dot(hidden, w_down, preferred_element_type=jnp.float32).reshape(
        sources, slot_count, -1
    )
    summed = lax.psum_scatter(
        partial_value.astype(jnp.bfloat16), "tp", scatter_dimension=2, tiled=True
    )
    returned = lax.all_to_all(summed, "sp", split_axis=0, concat_axis=0, tiled=True)
    flat_back = returned.reshape(experts * capacity, feat_block)
    picked = flat_back[slot_index].astype(jnp.float32).reshape(tok_rows, 2, feat_block)
    moe_sum = jnp.sum(route_weights[:, :, None] * picked, 1)
    own_cols = lax.dynamic_slice_in_dim(mixed_rows, offset, feat_block, 1).astype(jnp.float32)
    pre_norm = residual_alpha * own_cols + moe_sum
    fin_sum, fin_square = lax.psum((jnp.sum(pre_norm, 1), jnp.sum(pre_norm * pre_norm, 1)), "tp")
    features = feat_block * lax.axis_size("tp")
    fin_mean = fin_sum[:, None] / features
    fin_var = fin_square[:, None] / features - fin_mean * fin_mean
    return ((pre_norm - fin_mean) * lax.rsqrt(fin_var + norm_eps) * final_gain).astype(jnp.bfloat16)


HALO = 32
TILE = 256
TURNS = (0, 4, 1, 6, 2, 5, 3, 7)
SIZES = (1, 2, 2, 2, 1)
PLAN = (
    ("D0", "D1", "D2", "S0", "F0", "D3", "D4"),
    ((), ("L2", "D6"), ("L1", "D5"), ("D7", "F2"), ("L4", "F1", "X0")),
    ((), ("L3",), ("F4", "L6"), (), ("F3", "L5")),
    (("X1",), (), ("F6", "L7"), ("R0",), ("F5", "R1")),
    (("X2",), ("R2",), (), (), ("F7", "R3")),
    (("X3",), ("R4",), (), (), ()),
    ("X4", "R5", "R6", "R7"),
)
F32 = jnp.float32
BF16 = jnp.bfloat16


def block_kernel(
    sp_n,
    tp_n,
    capacity,
    taps,
    glu_value_hbm,
    glu_gate_hbm,
    ids_hbm,
    conv_kernel_hbm,
    conv_gain_hbm,
    out_weight_hbm,
    residual_hbm,
    mix_gain_hbm,
    routes_hbm,
    weights_hbm,
    gate_hbm,
    up_hbm,
    down_hbm,
    final_gain_hbm,
    out,
    glu_value,
    glu_gate,
    ids_row,
    conv_kernel,
    conv_gain,
    mix_gain,
    routes_row,
    weights_row,
    final_gain,
    w_out,
    resid,
    w_gate,
    w_up,
    w_down,
    rim_out,
    rim_in,
    rim_ids,
    by_row,
    by_col,
    ext,
    ext_ids,
    fil,
    stat_out,
    stat_in,
    mix_pp,
    mix_a,
    mix_s,
    mix_b,
    plain,
    raw,
    mixed,
    ready,
    note_out,
    note_in,
    outbox,
    rows_in,
    hidden,
    part_pp,
    part_a,
    part_s,
    part_b,
    part_own,
    back_out,
    back_in,
    small_sem,
    load_sem,
    halo_sem,
    stat_send,
    stat_recv,
    mix_send,
    mix_recv,
    note_send,
    note_recv,
    disp_send,
    disp_recv,
    ag_send,
    ag_recv,
    part_send,
    part_recv,
    cross_send,
    cross_recv,
    back_send,
    back_recv,
):
    tok, chan = glu_value.shape
    feat = final_gain_hbm.shape[1]
    ff = hidden.shape[2]
    y_n = tp_n // 2
    sp = lax.axis_index("sp")
    tp = lax.axis_index("tp")
    y = tp // 2
    core = tp % 2
    partner = y * 2 + (1 - core)
    groups = len(SIZES)
    begins = [sum(SIZES[:g]) for g in range(groups)]
    members = [range(begins[g], begins[g] + SIZES[g]) for g in range(groups)]
    pending = []

    def y_at(k):
        return lax.rem(y + k, y_n)

    def peer(p):
        to, bit = sp, 1
        while bit < sp_n:
            if TURNS[p] & bit:
                to = to + bit - 2 * bit * lax.rem(lax.div(sp, bit), 2)
            bit *= 2
        return to

    def feat_cols(block):
        return pl.ds(pl.multiple_of(block * feat, feat), feat)

    def remote(src, dst, send, recv, axis, to):
        return pltpu.make_async_remote_copy(
            src_ref=src,
            dst_ref=dst,
            send_sem=send,
            recv_sem=recv,
            device_id={axis: to},
            device_id_type=pl.DeviceIdType.MESH,
        )

    def send(*args):
        copy = remote(*args)
        copy.start()
        pending.append(copy)

    def arrived(dst, recv, send_sem, axis, to):
        remote(dst, dst, send_sem, recv, axis, to).wait_recv()

    barrier = pltpu.get_barrier_semaphore()
    for k in range(1, sp_n):
        pl.semaphore_signal(
            barrier, inc=1, device_id={"sp": lax.rem(sp + k, sp_n)},
            device_id_type=pl.DeviceIdType.MESH,
        )
    for k in range(1, tp_n):
        pl.semaphore_signal(
            barrier, inc=1, device_id={"tp": lax.rem(tp + k, tp_n)},
            device_id_type=pl.DeviceIdType.MESH,
        )

    smalls = []
    for i, (src, dst) in enumerate(
        (
            (ids_hbm, ids_row),
            (routes_hbm, routes_row),
            (weights_hbm, weights_row),
            (glu_value_hbm, glu_value),
            (glu_gate_hbm, glu_gate),
            (conv_kernel_hbm, conv_kernel),
            (conv_gain_hbm, conv_gain),
            (mix_gain_hbm, mix_gain),
            (final_gain_hbm, final_gain),
        )
    ):
        copy = pltpu.make_async_copy(src, dst, small_sem.at[i])
        copy.start()
        smalls.append(copy)
    for copy in smalls:
        copy.wait()
    loads = []
    for i, (src, dst) in enumerate(
        (
            (out_weight_hbm, w_out),
            (residual_hbm.at[:, feat_cols(tp)], resid),
            (gate_hbm.at[0], w_gate),
            (up_hbm.at[0], w_up),
            (down_hbm.at[0], w_down),
        )
    ):
        copy = pltpu.make_async_copy(src, dst, load_sem.at[i])
        copy.start()
        loads.append(copy)

    lanes = 128
    wide = by_row.shape[1]
    by_row[...] = jnp.zeros_like(by_row)
    by_row[0:1, 0:tok] = ids_row[...].astype(F32)
    by_row[1:3, 0:tok] = routes_row[...].astype(F32)
    by_row[3:5, 0:tok] = weights_row[...]
    by_col[...] = jnp.concatenate([by_row[...], jnp.zeros((lanes - 8, wide), F32)], 0).T[:tok]
    ext_ids[HALO:, :] = jnp.broadcast_to(by_col[:, 0:1].astype(jnp.int32), (tok, lanes))

    value = glu_value[...].astype(F32)
    gated = (value * jax.nn.sigmoid(glu_gate[...].astype(F32))).astype(BF16)
    ext[HALO:, :] = gated.astype(F32)
    rim_out[...] = gated[tok - HALO :]

    lower = (
        lax.broadcasted_iota(jnp.int32, (tok, tok), 1)
        < lax.broadcasted_iota(jnp.int32, (tok, tok), 0)
    )
    upper = (
        lax.broadcasted_iota(jnp.int32, (tok, tok), 0)
        < lax.broadcasted_iota(jnp.int32, (tok, tok), 1)
    )
    e_lane = lax.broadcasted_iota(jnp.int32, (tok, lanes), 1)
    one_lane = lax.broadcasted_iota(jnp.int32, (1, lanes), 1)
    subs = -(-sp_n // 16) * 16
    e_sub = lax.broadcasted_iota(jnp.int32, (subs, tok), 0)
    lane_expert = jnp.full((1, lanes), -1, jnp.int32)
    sub_expert = jnp.full((subs, tok), -1, jnp.int32)
    for r in range(sp_n):
        lane_expert = jnp.where(one_lane == r, peer(r), lane_expert)
        sub_expert = jnp.where(e_sub == r, peer(r), sub_expert)
    lane_expert = lane_expert.astype(F32)
    m0 = (by_col[:, 1:2] == lane_expert).astype(F32)
    m1 = (by_col[:, 2:3] == lane_expert).astype(F32)
    rank = jnp.dot(lower.astype(F32).astype(BF16), (m0 + m1).astype(BF16), preferred_element_type=F32)
    place = rank + (e_lane * capacity).astype(F32)
    slot_col0 = jnp.sum(m0 * place, 1, keepdims=True).astype(jnp.int32)
    slot_col1 = jnp.sum(m1 * place, 1, keepdims=True).astype(jnp.int32)
    spaced = rank + (e_lane * lanes).astype(F32)
    wide_col0 = jnp.sum(m0 * spaced, 1, keepdims=True).astype(jnp.int32)
    wide_col1 = jnp.sum(m1 * spaced, 1, keepdims=True).astype(jnp.int32)
    n0 = (routes_row[0:1, :] == sub_expert).astype(F32)
    n1 = (routes_row[1:2, :] == sub_expert).astype(F32)
    rank_r = jnp.dot((n0 + n1).astype(BF16), upper.astype(F32).astype(BF16), preferred_element_type=F32)
    place_r = rank_r + (e_sub * capacity).astype(F32)
    slot_row0 = jnp.sum(n0 * place_r, 0, keepdims=True).astype(jnp.int32)
    slot_row1 = jnp.sum(n1 * place_r, 0, keepdims=True).astype(jnp.int32)

    pl.semaphore_wait(barrier, sp_n + tp_n - 2)

    right = lax.rem(sp + 1, sp_n)
    halo = [
        remote(src, dst, halo_sem.at[0, i], halo_sem.at[1, i], "sp", right)
        for i, (src, dst) in enumerate(
            ((rim_out, rim_in), (ext_ids.at[pl.ds(tok, HALO)], rim_ids))
        )
    ]

    @pl.when(sp < sp_n - 1)
    def _():
        for copy in halo:
            copy.start()

    kern = conv_kernel[...].astype(F32)
    lane_blocks = chan // lanes

    def convolve(at):
        own = ext_ids[HALO + at : 2 * HALO + at, :]
        acc = [jnp.zeros((HALO, lanes), F32) for _ in range(lane_blocks)]
        for lag in range(taps):
            begin = HALO + at - lag
            same = ext_ids[begin : begin + HALO, :] == own
            for b in range(lane_blocks):
                part = ext[begin : begin + HALO, b * lanes : (b + 1) * lanes]
                acc[b] = acc[b] + jnp.where(same, part, 0.0) * kern[lag : lag + 1, b * lanes : (b + 1) * lanes]
        for b in range(lane_blocks):
            fil[at : at + HALO, b * lanes : (b + 1) * lanes] = acc[b]

    for at in range(HALO, tok, HALO):
        convolve(at)

    @pl.when(sp == 0)
    def _():
        ext[:HALO, :] = jnp.zeros((HALO, chan), F32)
        ext_ids[:HALO, :] = jnp.full((HALO, lanes), -1, jnp.int32)

    @pl.when(sp > 0)
    def _():
        for copy in halo:
            copy.wait_recv()
        ext[:HALO, :] = rim_in[...].astype(F32)
        ext_ids[:HALO, :] = rim_ids[...]

    convolve(0)

    def stats_out(i, value):
        row_sum = jnp.sum(value, 1, keepdims=True)
        row_square = jnp.sum(value * value, 1, keepdims=True)
        packed = jnp.where(e_lane == 0, row_sum, jnp.where(e_lane == 1, row_square, 0.0))
        packed = jnp.concatenate([packed, jnp.zeros((wide - tok, lanes), F32)], 0)
        stat_out[i] = packed.T[:8]
        for k in range(1, tp_n):
            send(
                stat_out.at[i], stat_in.at[i, k], stat_send.at[i, k], stat_recv.at[i, k],
                "tp", lax.rem(tp + k, tp_n),
            )

    def stats_in(i, width):
        total = stat_out[i]
        for k in range(1, tp_n):
            arrived(stat_in.at[i, k], stat_recv.at[i, k], stat_send.at[i, k], "tp", partner)
            total = total + stat_in[i, k]
        mean = total[0:1] / width
        var = total[1:2] / width - mean * mean
        return mean, lax.rsqrt(var + norm_eps)

    row_of = lax.broadcasted_iota(jnp.int32, (8, wide), 0)

    def columns(rows, count):
        rows = jnp.concatenate([rows, jnp.zeros((lanes - 8, rows.shape[1]), F32)], 0)
        return rows.T[:count]

    def stats(i, value, width):
        stats_out(i, value)
        mean, scale = stats_in(i, width)
        both = columns(jnp.where(row_of == 0, mean, jnp.where(row_of == 1, scale, 0.0)), tok)
        return both[:, 0:1], both[:, 1:2]

    filtered = fil[...]
    mean, scale = stats(0, filtered, chan * tp_n)
    normed = (filtered - mean) * scale * conv_gain[...]
    conv_out = (normed * jax.nn.sigmoid(normed)).astype(BF16)

    loads[0].wait()
    order = list(range(1, y_n)) + [0]
    for k in order:
        cols = feat_cols(2 * y_at(k) + 1 - core)
        mix_pp[k] = jnp.dot(conv_out, w_out[:, cols], preferred_element_type=F32).astype(BF16)
        send(mix_pp.at[k], mix_a.at[k], mix_send.at[0, k], mix_recv.at[0, k], "tp", partner)
    own_mix = None
    for k in order:
        cols = feat_cols(2 * y_at(k) + core)
        value = jnp.dot(conv_out, w_out[:, cols], preferred_element_type=F32)
        arrived(mix_a.at[k], mix_recv.at[0, k], mix_send.at[0, k], "tp", partner)
        value = value + mix_a[k].astype(F32)
        if k:
            mix_s[k] = value.astype(BF16)
            send(
                mix_s.at[k], mix_b.at[k], mix_send.at[1, k], mix_recv.at[1, k],
                "tp", 2 * y_at(k) + core,
            )
        else:
            own_mix = value
    loads[1].wait()
    pre = own_mix + residual_alpha * resid[...].astype(F32)
    for k in range(1, y_n):
        arrived(mix_b.at[k], mix_recv.at[1, k], mix_send.at[1, k], "tp", partner)
        pre = pre + mix_b[k].astype(F32)
    plain[...] = pre
    raw[...] = pre.astype(BF16)
    stats_out(1, pre)

    def spread(d):
        block = rows_in.at[tp, d]
        send(block, block, ag_send.at[0, d], ag_recv.at[0, d], "tp", partner)
        for k in range(1, y_n):
            send(
                block, block, ag_send.at[k, d], ag_recv.at[k, d],
                "tp", 2 * y_at(k) + core,
            )

    def pass_on(d):
        for k in range(1, y_n):
            block = rows_in.at[2 * y_at(y_n - k) + core, d]
            arrived(block, ag_recv.at[k, d], ag_send.at[k, d], "tp", partner)
            send(
                block, block, ag_send.at[y_n - 1 + k, d], ag_recv.at[y_n - 1 + k, d],
                "tp", partner,
            )

    def gathered(d):
        block = rows_in.at[partner, d]
        arrived(block, ag_recv.at[0, d], ag_send.at[0, d], "tp", partner)
        for k in range(1, y_n):
            block = rows_in.at[2 * y_at(y_n - k) + 1 - core, d]
            arrived(block, ag_recv.at[y_n - 1 + k, d], ag_send.at[y_n - 1 + k, d], "tp", partner)

    def dispatch(p):
        s_at = lax.broadcasted_iota(jnp.int32, (capacity, tok), 0) + p * capacity
        table = jnp.logical_or(s_at == slot_row0, s_at == slot_row1).astype(F32).astype(BF16)
        block = jnp.dot(table, raw[...], preferred_element_type=F32).astype(BF16)
        if p:
            outbox[p] = block
            send(
                outbox.at[p], rows_in.at[tp, p], disp_send.at[p], disp_recv.at[p],
                "sp", peer(p),
            )
        else:
            rows_in[tp, 0] = block
            spread(0)

    def describe(_):
        mean, scale = stats_in(1, feat * tp_n)
        both = columns(jnp.where(row_of == 0, mean, jnp.where(row_of == 1, scale, 0.0)), tok)
        mixed[...] = (
            (plain[...] - both[:, 0:1]) * both[:, 1:2] * mix_gain[:, feat_cols(tp)]
        ).astype(BF16)
        mean_top = mean.astype(BF16).astype(F32)
        scale_top = scale.astype(BF16).astype(F32)
        rows = jnp.zeros((8, wide), F32)
        for at, row in enumerate((mean_top, mean - mean_top, scale_top, scale - scale_top)):
            rows = jnp.where(row_of == at, row, rows)
        w_lane = lax.broadcasted_iota(jnp.int32, (tok, sp_n * lanes), 1)
        takes = jnp.logical_or(w_lane == wide_col0, w_lane == wide_col1).astype(F32).astype(BF16)
        told = jnp.dot(rows[:, :tok].astype(BF16), takes, preferred_element_type=F32)
        for p in range(sp_n):
            block = told[:, p * lanes : (p + 1) * lanes]
            if p:
                note_out[p] = block
                send(note_out.at[p], note_in.at[p], note_send.at[p], note_recv.at[p], "sp", peer(p))
            else:
                note_in[0] = block

    def normalize(g, i, p):
        if p:
            arrived(note_in.at[p], note_recv.at[p], note_send.at[p], "sp", right)
        note = columns(note_in[p], capacity)
        mean = note[:, 0:1] + note[:, 1:2]
        scale = note[:, 2:3] + note[:, 3:4]
        for j in range(tp_n):
            cols = pl.ds(j * feat, feat)
            value = (rows_in[j, p].astype(F32) - mean) * scale * mix_gain[:, cols]
            ready[i * capacity : (i + 1) * capacity, cols] = value.astype(BF16)

    def landed(p):
        arrived(rows_in.at[tp, p], disp_recv.at[p], disp_send.at[p], "sp", right)
        spread(p)

    def gate_up(g, lo, hi):
        cols = pl.ds(lo * TILE, (hi - lo) * TILE)
        rows = SIZES[g] * capacity
        x = ready[:rows]
        gate = jnp.dot(x, w_gate[:, cols], preferred_element_type=F32)
        up = jnp.dot(x, w_up[:, cols], preferred_element_type=F32)
        hidden[g, :rows, cols] = (gate * jax.nn.sigmoid(gate) * up).astype(BF16)

    def down(g):
        rows = pl.ds(0, SIZES[g] * capacity)

        def part(block):
            return jnp.dot(hidden[g, rows], w_down[:, feat_cols(block)], preferred_element_type=F32)

        for k in order:
            part_pp[g, k, rows] = part(2 * y_at(k) + 1 - core).astype(BF16)
            send(
                part_pp.at[g, k, rows], part_a.at[g, k, rows],
                part_send.at[g, k], part_recv.at[g, k], "tp", partner,
            )
            part_own[g, k, rows] = part(2 * y_at(k) + core)

    def cross(g):
        rows = pl.ds(0, SIZES[g] * capacity)
        for k in order:
            arrived(
                part_a.at[g, k, rows], part_recv.at[g, k], part_send.at[g, k], "tp", partner
            )
            if not k:
                continue
            part_s[g, k, rows] = (part_own[g, k, rows] + part_a[g, k, rows].astype(F32)).astype(BF16)
            for p in sorted(members[g], key=lambda p: -TURNS[p]):
                i = p - begins[g]
                one = pl.ds(i * capacity, capacity)
                send(
                    part_s.at[g, k, one], part_b.at[g, k, one],
                    cross_send.at[g, k, i], cross_recv.at[g, k, i],
                    "tp", 2 * y_at(k) + core,
                )

    def finish(p):
        g = [p in m for m in members].index(True)
        i = p - begins[g]
        rows = pl.ds(i * capacity, capacity)
        value = part_own[g, 0, rows, :] + part_a[g, 0, rows, :].astype(F32)
        for k in range(1, y_n):
            arrived(
                part_b.at[g, k, rows], cross_recv.at[g, k, i], cross_send.at[g, k, i],
                "tp", partner,
            )
            value = value + part_b[g, k, rows, :].astype(F32)
        if p:
            back_out[p] = value.astype(BF16)
            send(
                back_out.at[p], back_in.at[p], back_send.at[p], back_recv.at[p],
                "sp", peer(p),
            )
        else:
            back_in[0] = value.astype(BF16)

    tiles = ff // TILE
    do = dict(D=dispatch, S=describe, L=landed, F=pass_on, R=finish, X=cross)

    def act(text):
        for word in text:
            do[word[0]](int(word[1:]))

    act(PLAN[0])
    loads[2].wait()
    loads[3].wait()
    for g in range(groups):
        for i, p in enumerate(members[g]):
            gathered(p)
            normalize(g, i, p)
        act(PLAN[1 + g][0])
        for n in range(0, tiles, 2):
            gate_up(g, n, min(n + 2, tiles))
            act(PLAN[1 + g][1 + n // 2])
        if g == 0:
            loads[4].wait()
        down(g)
        act(PLAN[1 + g][4])
    act(PLAN[-1])

    def combine(lo, hi):
        for p in range(max(lo, 1), hi):
            arrived(back_in.at[p], back_recv.at[p], back_send.at[p], "sp", right)
        slots = (hi - lo) * capacity
        rows = back_in[lo:hi].reshape(slots, feat)
        s_lane = lax.broadcasted_iota(jnp.int32, (tok, slots), 1) + lo * capacity
        pick0 = jnp.dot((s_lane == slot_col0).astype(F32).astype(BF16), rows, preferred_element_type=F32)
        pick1 = jnp.dot((s_lane == slot_col1).astype(F32).astype(BF16), rows, preferred_element_type=F32)
        return by_col[:, 3:4] * pick0 + by_col[:, 4:5] * pick1

    moe = combine(0, begins[-1]) + combine(begins[-1], sp_n)
    pre = residual_alpha * mixed[...].astype(F32) + moe
    mean, scale = stats(2, pre, feat * tp_n)
    out[...] = ((pre - mean) * scale * final_gain[...]).astype(BF16)
    for copy in pending:
        copy.wait_send()

    @pl.when(sp < sp_n - 1)
    def _():
        for copy in halo:
            copy.wait_send()


def local_kernel(
    glu_value,
    glu_gate,
    doc_ids,
    conv_kernel,
    conv_gain,
    out_weight,
    residual,
    mix_gain,
    routes,
    route_weights,
    expert_gate,
    expert_up,
    expert_down,
    final_gain,
):
    sp_n, tp_n = lax.axis_size("sp"), lax.axis_size("tp")
    tok, chan = glu_value.shape
    feat = final_gain.shape[0]
    width, ff = expert_gate.shape[1:]
    capacity = 4 * tok // sp_n
    y_n = tp_n // 2
    groups, most = len(SIZES), max(SIZES)
    rows = most * capacity
    wide = -(-tok // 128) * 128
    vmem = pl.BlockSpec(memory_space=pltpu.VMEM)
    hbm = pl.BlockSpec(memory_space=pl.ANY)
    dma = pltpu.SemaphoreType.DMA
    scratch = [
        pltpu.VMEM((tok, chan), BF16),
        pltpu.VMEM((tok, chan), BF16),
        pltpu.VMEM((1, tok), jnp.int32),
        pltpu.VMEM(conv_kernel.shape, BF16),
        pltpu.VMEM((1, chan), F32),
        pltpu.VMEM((1, width), F32),
        pltpu.VMEM((2, tok), jnp.int32),
        pltpu.VMEM((2, tok), F32),
        pltpu.VMEM((1, feat), F32),
        pltpu.VMEM((chan, width), BF16),
        pltpu.VMEM((tok, feat), BF16),
        pltpu.VMEM((width, ff), BF16),
        pltpu.VMEM((width, ff), BF16),
        pltpu.VMEM((ff, width), BF16),
        pltpu.VMEM((HALO, chan), BF16),
        pltpu.VMEM((HALO, chan), BF16),
        pltpu.VMEM((HALO, 128), jnp.int32),
        pltpu.VMEM((8, wide), F32),
        pltpu.VMEM((tok, 128), F32),
        pltpu.VMEM((HALO + tok, chan), F32),
        pltpu.VMEM((HALO + tok, 128), jnp.int32),
        pltpu.VMEM((tok, chan), F32),
        pltpu.VMEM((3, 8, wide), F32),
        pltpu.VMEM((3, tp_n, 8, wide), F32),
        pltpu.VMEM((y_n, tok, feat), BF16),
        pltpu.VMEM((y_n, tok, feat), BF16),
        pltpu.VMEM((y_n, tok, feat), BF16),
        pltpu.VMEM((y_n, tok, feat), BF16),
        pltpu.VMEM((tok, feat), F32),
        pltpu.VMEM((tok, feat), BF16),
        pltpu.VMEM((tok, feat), BF16),
        pltpu.VMEM((rows, width), BF16),
        pltpu.VMEM((sp_n, 8, 128), F32),
        pltpu.VMEM((sp_n, 8, 128), F32),
        pltpu.VMEM((sp_n, capacity, feat), BF16),
        pltpu.VMEM((tp_n, sp_n, capacity, feat), BF16),
        pltpu.VMEM((groups, rows, ff), BF16),
        pltpu.VMEM((groups, y_n, rows, feat), BF16),
        pltpu.VMEM((groups, y_n, rows, feat), BF16),
        pltpu.VMEM((groups, y_n, rows, feat), BF16),
        pltpu.VMEM((groups, y_n, rows, feat), BF16),
        pltpu.VMEM((groups, y_n, rows, feat), F32),
        pltpu.VMEM((sp_n, capacity, feat), BF16),
        pltpu.VMEM((sp_n, capacity, feat), BF16),
        dma((9,)),
        dma((5,)),
        dma((2, 2)),
        dma((3, tp_n)),
        dma((3, tp_n)),
        dma((2, y_n)),
        dma((2, y_n)),
        dma((sp_n,)),
        dma((sp_n,)),
        dma((sp_n,)),
        dma((sp_n,)),
        dma((2 * y_n - 1, sp_n)),
        dma((2 * y_n - 1, sp_n)),
        dma((groups, y_n)),
        dma((groups, y_n)),
        dma((groups, y_n, most)),
        dma((groups, y_n, most)),
        dma((sp_n,)),
        dma((sp_n,)),
    ]
    return pl.pallas_call(
        functools.partial(block_kernel, sp_n, tp_n, capacity, conv_kernel.shape[0]),
        out_shape=pltpu.VMEM((tok, feat), BF16),
        in_specs=[hbm] * 14,
        out_specs=vmem,
        scratch_shapes=scratch,
        compiler_params=pltpu.CompilerParams(
            collective_id=0, has_side_effects=True, vmem_limit_bytes=60 * 1024 * 1024
        ),
    )(
        glu_value,
        glu_gate,
        doc_ids[None, :],
        conv_kernel,
        conv_gain[None, :],
        out_weight,
        residual,
        mix_gain[None, :],
        routes.T,
        route_weights.T,
        expert_gate,
        expert_up,
        expert_down,
        final_gain[None, :],
    )


def local(*args):
    sp_n, tp_n = lax.axis_size("sp"), lax.axis_size("tp")
    tok, chan = args[0].shape
    ff = args[10].shape[2]
    feat = args[13].shape[0]
    aligned = (
        chan % 128 == 0
        and feat % TILE == 0
        and ff % TILE == 0
        and (4 * tok // sp_n) % 32 == 0
        and 4 * tok // sp_n <= 128
        and tok % HALO == 0
        and args[3].shape[0] <= HALO
        and tp_n % 2 == 0
        and tp_n > 2
        and sp_n == len(TURNS)
        and ff <= 2 * TILE * (len(PLAN[1]) - 2)
        and args[10].shape[0] == 1
    )
    return (local_kernel if aligned else local_plain)(*args)


def solution(mesh):
    return jax.shard_map(
        local,
        mesh=mesh,
        in_specs=(
            P("sp", "tp"),
            P("sp", "tp"),
            P("sp"),
            P(None, "tp"),
            P("tp"),
            P("tp", None),
            P("sp", None),
            P(),
            P("sp", None),
            P("sp", None),
            P("sp", None, "tp"),
            P("sp", None, "tp"),
            P("sp", "tp", None),
            P("tp"),
        ),
        out_specs=P("sp", "tp"),
        check_vma=False,
    )
```

```python
import functools

import jax
import jax.numpy as jnp
from jax import lax
from jax.experimental import pallas as pl
from jax.experimental.pallas import tpu as pltpu
from jax.sharding import PartitionSpec as P

residual_alpha = 1.41421356
norm_eps = 1e-05


def from_behind(value, axis, by):
    peers = lax.axis_size(axis)
    pairs = [(i, i + by) for i in range(peers) if 0 <= i + by < peers]
    return lax.ppermute(value, axis, pairs)


def scaled_norm(pre_norm, gain):
    row_mean = jnp.mean(pre_norm, -1, keepdims=True)
    row_var = jnp.mean(pre_norm * pre_norm, -1, keepdims=True) - row_mean * row_mean
    return (pre_norm - row_mean) * lax.rsqrt(row_var + norm_eps) * gain


def local_plain(
    glu_value,
    glu_gate,
    doc_ids,
    conv_kernel,
    conv_gain,
    out_weight,
    residual,
    mix_gain,
    routes,
    route_weights,
    expert_gate,
    expert_up,
    expert_down,
    final_gain,
):
    tok_rows = glu_value.shape[0]
    rim_len = conv_kernel.shape[0] - 1
    channels = glu_value.shape[1] * lax.axis_size("tp")
    gated_rows = (
        glu_value.astype(jnp.float32) * jax.nn.sigmoid(glu_gate.astype(jnp.float32))
    ).astype(jnp.bfloat16)
    rim_rows, rim_ids = from_behind(
        (gated_rows[tok_rows - rim_len :], doc_ids[tok_rows - rim_len :]), "sp", 1
    )
    extended = jnp.concatenate([rim_rows, gated_rows], 0).astype(jnp.float32)
    ext_ids = jnp.concatenate([rim_ids, doc_ids], 0)
    kernel = conv_kernel.astype(jnp.float32)
    filtered = jnp.zeros(gated_rows.shape, jnp.float32)
    for shift_by in range(rim_len + 1):
        begin_at = rim_len - shift_by
        same_doc = (ext_ids[begin_at : begin_at + tok_rows] == doc_ids)[:, None]
        filtered = (
            filtered
            + jnp.where(same_doc, extended[begin_at : begin_at + tok_rows], 0.0) * kernel[shift_by]
        )
    row_sum, row_square = lax.psum((jnp.sum(filtered, 1), jnp.sum(filtered * filtered, 1)), "tp")
    row_mean = row_sum[:, None] / channels
    row_var = row_square[:, None] / channels - row_mean * row_mean
    conv_out = jax.nn.silu(
        (filtered - row_mean) * lax.rsqrt(row_var + norm_eps) * conv_gain
    ).astype(jnp.bfloat16)
    mix_total = lax.psum(
        jnp.dot(conv_out, out_weight, preferred_element_type=jnp.float32).astype(jnp.bfloat16), "tp"
    ).astype(jnp.float32)
    mixed_rows = scaled_norm(
        residual_alpha * residual.astype(jnp.float32) + mix_total, mix_gain
    ).astype(jnp.bfloat16)
    experts = expert_gate.shape[0] * lax.axis_size("sp")
    capacity = 4 * tok_rows // experts
    chosen = routes.reshape(-1)
    member = (chosen[:, None] == jnp.arange(experts, dtype=jnp.int32)[None, :]).astype(jnp.int32)
    earlier = jnp.cumsum(member, 0) - member
    slot_index = chosen * capacity + jnp.sum(earlier * member, 1)
    dispatch_table = jnp.any(
        jnp.arange(experts * capacity, dtype=jnp.int32)[:, None, None]
        == slot_index.reshape(tok_rows, 2)[None],
        -1,
    ).astype(jnp.bfloat16)
    feat_block = mixed_rows.shape[1] // lax.axis_size("tp")
    offset = lax.axis_index("tp") * feat_block
    w_gate = expert_gate[0]
    w_up = expert_up[0]
    w_down = expert_down[0]
    row_slice = lax.dynamic_slice_in_dim(mixed_rows, offset, feat_block, 1)
    outgoing = (
        jnp.dot(dispatch_table, row_slice, preferred_element_type=jnp.float32)
        .astype(jnp.bfloat16)
        .reshape(experts, capacity, feat_block)
    )
    arrived = lax.all_to_all(outgoing, "sp", split_axis=0, concat_axis=0, tiled=True)
    sources, slot_count, part_width = arrived.shape
    flat_rows = arrived.reshape(sources * slot_count, part_width)
    col_piece = lax.all_gather(flat_rows, "tp", axis=1, tiled=True)
    gate_proj = jnp.dot(col_piece, w_gate, preferred_element_type=jnp.float32)
    up_proj = jnp.dot(col_piece, w_up, preferred_element_type=jnp.float32)
    hidden = (jax.nn.silu(gate_proj) * up_proj).astype(jnp.bfloat16)
    partial_value = jnp.dot(hidden, w_down, preferred_element_type=jnp.float32).reshape(
        sources, slot_count, -1
    )
    summed = lax.psum_scatter(
        partial_value.astype(jnp.bfloat16), "tp", scatter_dimension=2, tiled=True
    )
    returned = lax.all_to_all(summed, "sp", split_axis=0, concat_axis=0, tiled=True)
    flat_back = returned.reshape(experts * capacity, feat_block)
    picked = flat_back[slot_index].astype(jnp.float32).reshape(tok_rows, 2, feat_block)
    moe_sum = jnp.sum(route_weights[:, :, None] * picked, 1)
    own_cols = lax.dynamic_slice_in_dim(mixed_rows, offset, feat_block, 1).astype(jnp.float32)
    pre_norm = residual_alpha * own_cols + moe_sum
    fin_sum, fin_square = lax.psum((jnp.sum(pre_norm, 1), jnp.sum(pre_norm * pre_norm, 1)), "tp")
    features = feat_block * lax.axis_size("tp")
    fin_mean = fin_sum[:, None] / features
    fin_var = fin_square[:, None] / features - fin_mean * fin_mean
    return ((pre_norm - fin_mean) * lax.rsqrt(fin_var + norm_eps) * final_gain).astype(jnp.bfloat16)


HALO = 32
TILE = 256
TURNS = (0, 4, 1, 6, 2, 5, 3, 7)
SIZES = (1, 2, 2, 2, 1)
PLAN = (
    ("D0", "D1", "D2", "S0", "F0", "D3", "D4"),
    ((), ("L2", "D6"), ("L1", "D5"), ("D7", "F2"), ("L4", "F1", "L3", "X0")),
    ((), ("L6",), ("F4",), ("L5",), ("F3",)),
    (("X1",), ("L7",), ("F6",), ("R0",), ("F5", "R1")),
    (("X2",), ("R2",), (), (), ("F7", "R3")),
    (("X3",), ("R4",), (), (), ()),
    ("X4", "R5", "R6", "R7"),
)
F32 = jnp.float32
BF16 = jnp.bfloat16


def block_kernel(
    sp_n,
    tp_n,
    capacity,
    taps,
    glu_value_hbm,
    glu_gate_hbm,
    ids_hbm,
    conv_kernel_hbm,
    conv_gain_hbm,
    out_weight_hbm,
    residual_hbm,
    mix_gain_hbm,
    routes_hbm,
    weights_hbm,
    gate_hbm,
    up_hbm,
    down_hbm,
    final_gain_hbm,
    out,
    glu_value,
    glu_gate,
    ids_row,
    conv_kernel,
    conv_gain,
    mix_gain,
    routes_row,
    weights_row,
    final_gain,
    w_out,
    resid,
    w_gate,
    w_up,
    w_down,
    rim_out,
    rim_in,
    rim_ids,
    by_row,
    by_col,
    ext,
    ext_ids,
    fil,
    stat_out,
    stat_in,
    mix_pp,
    mix_a,
    mix_s,
    mix_b,
    plain,
    raw,
    mixed,
    ready,
    note_out,
    note_in,
    outbox,
    rows_in,
    hidden,
    part_pp,
    part_a,
    part_s,
    part_b,
    part_own,
    back_out,
    back_in,
    small_sem,
    load_sem,
    halo_sem,
    stat_send,
    stat_recv,
    mix_send,
    mix_recv,
    note_send,
    note_recv,
    disp_send,
    disp_recv,
    ag_send,
    ag_recv,
    part_send,
    part_recv,
    cross_send,
    cross_recv,
    back_send,
    back_recv,
):
    tok, chan = glu_value.shape
    feat = final_gain_hbm.shape[1]
    ff = hidden.shape[2]
    y_n = tp_n // 2
    sp = lax.axis_index("sp")
    tp = lax.axis_index("tp")
    y = tp // 2
    core = tp % 2
    partner = y * 2 + (1 - core)
    groups = len(SIZES)
    begins = [sum(SIZES[:g]) for g in range(groups)]
    members = [range(begins[g], begins[g] + SIZES[g]) for g in range(groups)]
    pending = []

    def y_at(k):
        return lax.rem(y + k, y_n)

    def peer(p):
        to, bit = sp, 1
        while bit < sp_n:
            if TURNS[p] & bit:
                to = to + bit - 2 * bit * lax.rem(lax.div(sp, bit), 2)
            bit *= 2
        return to

    def feat_cols(block):
        return pl.ds(pl.multiple_of(block * feat, feat), feat)

    def remote(src, dst, send, recv, axis, to):
        return pltpu.make_async_remote_copy(
            src_ref=src,
            dst_ref=dst,
            send_sem=send,
            recv_sem=recv,
            device_id={axis: to},
            device_id_type=pl.DeviceIdType.MESH,
        )

    def send(*args):
        copy = remote(*args)
        copy.start()
        pending.append(copy)

    def arrived(dst, recv, send_sem, axis, to):
        remote(dst, dst, send_sem, recv, axis, to).wait_recv()

    barrier = pltpu.get_barrier_semaphore()
    for k in range(1, sp_n):
        pl.semaphore_signal(
            barrier, inc=1, device_id={"sp": lax.rem(sp + k, sp_n)},
            device_id_type=pl.DeviceIdType.MESH,
        )
    for k in range(1, tp_n):
        pl.semaphore_signal(
            barrier, inc=1, device_id={"tp": lax.rem(tp + k, tp_n)},
            device_id_type=pl.DeviceIdType.MESH,
        )

    smalls = []
    for i, (src, dst) in enumerate(
        (
            (ids_hbm, ids_row),
            (routes_hbm, routes_row),
            (weights_hbm, weights_row),
            (glu_value_hbm, glu_value),
            (glu_gate_hbm, glu_gate),
            (conv_kernel_hbm, conv_kernel),
            (conv_gain_hbm, conv_gain),
            (mix_gain_hbm, mix_gain),
            (final_gain_hbm, final_gain),
        )
    ):
        copy = pltpu.make_async_copy(src, dst, small_sem.at[i])
        copy.start()
        smalls.append(copy)
    for copy in smalls:
        copy.wait()
    loads = []
    for i, (src, dst) in enumerate(
        (
            (out_weight_hbm, w_out),
            (residual_hbm.at[:, feat_cols(tp)], resid),
            (gate_hbm.at[0], w_gate),
            (up_hbm.at[0], w_up),
            (down_hbm.at[0], w_down),
        )
    ):
        copy = pltpu.make_async_copy(src, dst, load_sem.at[i])
        copy.start()
        loads.append(copy)

    lanes = 128
    wide = by_row.shape[1]
    by_row[...] = jnp.zeros_like(by_row)
    by_row[0:1, 0:tok] = ids_row[...].astype(F32)
    by_row[1:3, 0:tok] = routes_row[...].astype(F32)
    by_row[3:5, 0:tok] = weights_row[...]
    by_col[...] = jnp.concatenate([by_row[...], jnp.zeros((lanes - 8, wide), F32)], 0).T[:tok]
    ext_ids[HALO:, :] = jnp.broadcast_to(by_col[:, 0:1].astype(jnp.int32), (tok, lanes))

    value = glu_value[...].astype(F32)
    gated = (value * jax.nn.sigmoid(glu_gate[...].astype(F32))).astype(BF16)
    ext[HALO:, :] = gated.astype(F32)
    rim_out[...] = gated[tok - HALO :]

    lower = (
        lax.broadcasted_iota(jnp.int32, (tok, tok), 1)
        < lax.broadcasted_iota(jnp.int32, (tok, tok), 0)
    )
    upper = (
        lax.broadcasted_iota(jnp.int32, (tok, tok), 0)
        < lax.broadcasted_iota(jnp.int32, (tok, tok), 1)
    )
    e_lane = lax.broadcasted_iota(jnp.int32, (tok, lanes), 1)
    one_lane = lax.broadcasted_iota(jnp.int32, (1, lanes), 1)
    subs = -(-sp_n // 16) * 16
    e_sub = lax.broadcasted_iota(jnp.int32, (subs, tok), 0)
    lane_expert = jnp.full((1, lanes), -1, jnp.int32)
    sub_expert = jnp.full((subs, tok), -1, jnp.int32)
    for r in range(sp_n):
        lane_expert = jnp.where(one_lane == r, peer(r), lane_expert)
        sub_expert = jnp.where(e_sub == r, peer(r), sub_expert)
    lane_expert = lane_expert.astype(F32)
    m0 = (by_col[:, 1:2] == lane_expert).astype(F32)
    m1 = (by_col[:, 2:3] == lane_expert).astype(F32)
    rank = jnp.dot(lower.astype(F32).astype(BF16), (m0 + m1).astype(BF16), preferred_element_type=F32)
    place = rank + (e_lane * capacity).astype(F32)
    slot_col0 = jnp.sum(m0 * place, 1, keepdims=True).astype(jnp.int32)
    slot_col1 = jnp.sum(m1 * place, 1, keepdims=True).astype(jnp.int32)
    spaced = rank + (e_lane * lanes).astype(F32)
    wide_col0 = jnp.sum(m0 * spaced, 1, keepdims=True).astype(jnp.int32)
    wide_col1 = jnp.sum(m1 * spaced, 1, keepdims=True).astype(jnp.int32)
    n0 = (routes_row[0:1, :] == sub_expert).astype(F32)
    n1 = (routes_row[1:2, :] == sub_expert).astype(F32)
    rank_r = jnp.dot((n0 + n1).astype(BF16), upper.astype(F32).astype(BF16), preferred_element_type=F32)
    place_r = rank_r + (e_sub * capacity).astype(F32)
    slot_row0 = jnp.sum(n0 * place_r, 0, keepdims=True).astype(jnp.int32)
    slot_row1 = jnp.sum(n1 * place_r, 0, keepdims=True).astype(jnp.int32)

    pl.semaphore_wait(barrier, sp_n + tp_n - 2)

    right = lax.rem(sp + 1, sp_n)
    halo = [
        remote(src, dst, halo_sem.at[0, i], halo_sem.at[1, i], "sp", right)
        for i, (src, dst) in enumerate(
            ((rim_out, rim_in), (ext_ids.at[pl.ds(tok, HALO)], rim_ids))
        )
    ]

    @pl.when(sp < sp_n - 1)
    def _():
        for copy in halo:
            copy.start()

    kern = conv_kernel[...].astype(F32)
    lane_blocks = chan // lanes

    def convolve(at):
        own = ext_ids[HALO + at : 2 * HALO + at, :]
        acc = [jnp.zeros((HALO, lanes), F32) for _ in range(lane_blocks)]
        for lag in range(taps):
            begin = HALO + at - lag
            same = ext_ids[begin : begin + HALO, :] == own
            for b in range(lane_blocks):
                part = ext[begin : begin + HALO, b * lanes : (b + 1) * lanes]
                acc[b] = acc[b] + jnp.where(same, part, 0.0) * kern[lag : lag + 1, b * lanes : (b + 1) * lanes]
        for b in range(lane_blocks):
            fil[at : at + HALO, b * lanes : (b + 1) * lanes] = acc[b]

    for at in range(HALO, tok, HALO):
        convolve(at)

    @pl.when(sp == 0)
    def _():
        ext[:HALO, :] = jnp.zeros((HALO, chan), F32)
        ext_ids[:HALO, :] = jnp.full((HALO, lanes), -1, jnp.int32)

    @pl.when(sp > 0)
    def _():
        for copy in halo:
            copy.wait_recv()
        ext[:HALO, :] = rim_in[...].astype(F32)
        ext_ids[:HALO, :] = rim_ids[...]

    convolve(0)

    def stats_out(i, value):
        row_sum = jnp.sum(value, 1, keepdims=True)
        row_square = jnp.sum(value * value, 1, keepdims=True)
        packed = jnp.where(e_lane == 0, row_sum, jnp.where(e_lane == 1, row_square, 0.0))
        packed = jnp.concatenate([packed, jnp.zeros((wide - tok, lanes), F32)], 0)
        stat_out[i] = packed.T[:8]
        for k in range(1, tp_n):
            send(
                stat_out.at[i], stat_in.at[i, k], stat_send.at[i, k], stat_recv.at[i, k],
                "tp", lax.rem(tp + k, tp_n),
            )

    def stats_in(i, width):
        total = stat_out[i]
        for k in range(1, tp_n):
            arrived(stat_in.at[i, k], stat_recv.at[i, k], stat_send.at[i, k], "tp", partner)
            total = total + stat_in[i, k]
        mean = total[0:1] / width
        var = total[1:2] / width - mean * mean
        return mean, lax.rsqrt(var + norm_eps)

    row_of = lax.broadcasted_iota(jnp.int32, (8, wide), 0)

    def columns(rows, count):
        rows = jnp.concatenate([rows, jnp.zeros((lanes - 8, rows.shape[1]), F32)], 0)
        return rows.T[:count]

    def stats(i, value, width):
        stats_out(i, value)
        mean, scale = stats_in(i, width)
        both = columns(jnp.where(row_of == 0, mean, jnp.where(row_of == 1, scale, 0.0)), tok)
        return both[:, 0:1], both[:, 1:2]

    filtered = fil[...]
    mean, scale = stats(0, filtered, chan * tp_n)
    normed = (filtered - mean) * scale * conv_gain[...]
    conv_out = (normed * jax.nn.sigmoid(normed)).astype(BF16)

    loads[0].wait()
    order = list(range(1, y_n)) + [0]
    for k in order:
        cols = feat_cols(2 * y_at(k) + 1 - core)
        mix_pp[k] = jnp.dot(conv_out, w_out[:, cols], preferred_element_type=F32).astype(BF16)
        send(mix_pp.at[k], mix_a.at[k], mix_send.at[0, k], mix_recv.at[0, k], "tp", partner)
    own_mix = None
    for k in order:
        cols = feat_cols(2 * y_at(k) + core)
        value = jnp.dot(conv_out, w_out[:, cols], preferred_element_type=F32)
        arrived(mix_a.at[k], mix_recv.at[0, k], mix_send.at[0, k], "tp", partner)
        value = value + mix_a[k].astype(F32)
        if k:
            mix_s[k] = value.astype(BF16)
            send(
                mix_s.at[k], mix_b.at[k], mix_send.at[1, k], mix_recv.at[1, k],
                "tp", 2 * y_at(k) + core,
            )
        else:
            own_mix = value
    loads[1].wait()
    pre = own_mix + residual_alpha * resid[...].astype(F32)
    for k in range(1, y_n):
        arrived(mix_b.at[k], mix_recv.at[1, k], mix_send.at[1, k], "tp", partner)
        pre = pre + mix_b[k].astype(F32)
    plain[...] = pre
    raw[...] = pre.astype(BF16)
    stats_out(1, pre)

    def spread(d):
        block = rows_in.at[tp, d]
        send(block, block, ag_send.at[0, d], ag_recv.at[0, d], "tp", partner)
        for k in range(1, y_n):
            send(
                block, block, ag_send.at[k, d], ag_recv.at[k, d],
                "tp", 2 * y_at(k) + core,
            )

    def pass_on(d):
        for k in range(1, y_n):
            block = rows_in.at[2 * y_at(y_n - k) + core, d]
            arrived(block, ag_recv.at[k, d], ag_send.at[k, d], "tp", partner)
            send(
                block, block, ag_send.at[y_n - 1 + k, d], ag_recv.at[y_n - 1 + k, d],
                "tp", partner,
            )

    def gathered(d):
        block = rows_in.at[partner, d]
        arrived(block, ag_recv.at[0, d], ag_send.at[0, d], "tp", partner)
        for k in range(1, y_n):
            block = rows_in.at[2 * y_at(y_n - k) + 1 - core, d]
            arrived(block, ag_recv.at[y_n - 1 + k, d], ag_send.at[y_n - 1 + k, d], "tp", partner)

    def dispatch(p):
        s_at = lax.broadcasted_iota(jnp.int32, (capacity, tok), 0) + p * capacity
        table = jnp.logical_or(s_at == slot_row0, s_at == slot_row1).astype(F32).astype(BF16)
        block = jnp.dot(table, raw[...], preferred_element_type=F32).astype(BF16)
        if p:
            outbox[p] = block
            send(
                outbox.at[p], rows_in.at[tp, p], disp_send.at[p], disp_recv.at[p],
                "sp", peer(p),
            )
        else:
            rows_in[tp, 0] = block
            spread(0)

    def describe(_):
        mean, scale = stats_in(1, feat * tp_n)
        both = columns(jnp.where(row_of == 0, mean, jnp.where(row_of == 1, scale, 0.0)), tok)
        mixed[...] = (
            (plain[...] - both[:, 0:1]) * both[:, 1:2] * mix_gain[:, feat_cols(tp)]
        ).astype(BF16)
        mean_top = mean.astype(BF16).astype(F32)
        scale_top = scale.astype(BF16).astype(F32)
        rows = jnp.zeros((8, wide), F32)
        for at, row in enumerate((mean_top, mean - mean_top, scale_top, scale - scale_top)):
            rows = jnp.where(row_of == at, row, rows)
        w_lane = lax.broadcasted_iota(jnp.int32, (tok, sp_n * lanes), 1)
        takes = jnp.logical_or(w_lane == wide_col0, w_lane == wide_col1).astype(F32).astype(BF16)
        told = jnp.dot(rows[:, :tok].astype(BF16), takes, preferred_element_type=F32)
        for p in range(sp_n):
            block = told[:, p * lanes : (p + 1) * lanes]
            if p:
                note_out[p] = block
                send(note_out.at[p], note_in.at[p], note_send.at[p], note_recv.at[p], "sp", peer(p))
            else:
                note_in[0] = block

    def normalize(g, i, p):
        if p:
            arrived(note_in.at[p], note_recv.at[p], note_send.at[p], "sp", right)
        note = columns(note_in[p], capacity)
        mean = note[:, 0:1] + note[:, 1:2]
        scale = note[:, 2:3] + note[:, 3:4]
        for j in range(tp_n):
            cols = pl.ds(j * feat, feat)
            value = (rows_in[j, p].astype(F32) - mean) * scale * mix_gain[:, cols]
            ready[i * capacity : (i + 1) * capacity, cols] = value.astype(BF16)

    def landed(p):
        arrived(rows_in.at[tp, p], disp_recv.at[p], disp_send.at[p], "sp", right)
        spread(p)

    def gate_up(g, lo, hi):
        cols = pl.ds(lo * TILE, (hi - lo) * TILE)
        rows = SIZES[g] * capacity
        x = ready[:rows]
        gate = jnp.dot(x, w_gate[:, cols], preferred_element_type=F32)
        up = jnp.dot(x, w_up[:, cols], preferred_element_type=F32)
        hidden[g, :rows, cols] = (gate * jax.nn.sigmoid(gate) * up).astype(BF16)

    def down(g):
        rows = pl.ds(0, SIZES[g] * capacity)

        def part(block):
            return jnp.dot(hidden[g, rows], w_down[:, feat_cols(block)], preferred_element_type=F32)

        for k in order:
            part_pp[g, k, rows] = part(2 * y_at(k) + 1 - core).astype(BF16)
            send(
                part_pp.at[g, k, rows], part_a.at[g, k, rows],
                part_send.at[g, k], part_recv.at[g, k], "tp", partner,
            )
            part_own[g, k, rows] = part(2 * y_at(k) + core)

    def cross(g):
        rows = pl.ds(0, SIZES[g] * capacity)
        for k in order:
            arrived(
                part_a.at[g, k, rows], part_recv.at[g, k], part_send.at[g, k], "tp", partner
            )
            if not k:
                continue
            part_s[g, k, rows] = (part_own[g, k, rows] + part_a[g, k, rows].astype(F32)).astype(BF16)
            for p in sorted(members[g], key=lambda p: -TURNS[p]):
                i = p - begins[g]
                one = pl.ds(i * capacity, capacity)
                send(
                    part_s.at[g, k, one], part_b.at[g, k, one],
                    cross_send.at[g, k, i], cross_recv.at[g, k, i],
                    "tp", 2 * y_at(k) + core,
                )

    def finish(p):
        g = [p in m for m in members].index(True)
        i = p - begins[g]
        rows = pl.ds(i * capacity, capacity)
        value = part_own[g, 0, rows, :] + part_a[g, 0, rows, :].astype(F32)
        for k in range(1, y_n):
            arrived(
                part_b.at[g, k, rows], cross_recv.at[g, k, i], cross_send.at[g, k, i],
                "tp", partner,
            )
            value = value + part_b[g, k, rows, :].astype(F32)
        if p:
            back_out[p] = value.astype(BF16)
            send(
                back_out.at[p], back_in.at[p], back_send.at[p], back_recv.at[p],
                "sp", peer(p),
            )
        else:
            back_in[0] = value.astype(BF16)

    tiles = ff // TILE
    do = dict(D=dispatch, S=describe, L=landed, F=pass_on, R=finish, X=cross)

    def act(text):
        for word in text:
            do[word[0]](int(word[1:]))

    act(PLAN[0])
    loads[2].wait()
    loads[3].wait()
    for g in range(groups):
        for i, p in enumerate(members[g]):
            gathered(p)
            normalize(g, i, p)
        act(PLAN[1 + g][0])
        for n in range(0, tiles, 2):
            gate_up(g, n, min(n + 2, tiles))
            act(PLAN[1 + g][1 + n // 2])
        if g == 0:
            loads[4].wait()
        down(g)
        act(PLAN[1 + g][4])
    act(PLAN[-1])

    def combine(lo, hi):
        for p in range(max(lo, 1), hi):
            arrived(back_in.at[p], back_recv.at[p], back_send.at[p], "sp", right)
        slots = (hi - lo) * capacity
        rows = back_in[lo:hi].reshape(slots, feat)
        s_lane = lax.broadcasted_iota(jnp.int32, (tok, slots), 1) + lo * capacity
        pick0 = jnp.dot((s_lane == slot_col0).astype(F32).astype(BF16), rows, preferred_element_type=F32)
        pick1 = jnp.dot((s_lane == slot_col1).astype(F32).astype(BF16), rows, preferred_element_type=F32)
        return by_col[:, 3:4] * pick0 + by_col[:, 4:5] * pick1

    moe = combine(0, begins[-1]) + combine(begins[-1], sp_n)
    pre = residual_alpha * mixed[...].astype(F32) + moe
    mean, scale = stats(2, pre, feat * tp_n)
    out[...] = ((pre - mean) * scale * final_gain[...]).astype(BF16)
    for copy in pending:
        copy.wait_send()

    @pl.when(sp < sp_n - 1)
    def _():
        for copy in halo:
            copy.wait_send()


def local_kernel(
    glu_value,
    glu_gate,
    doc_ids,
    conv_kernel,
    conv_gain,
    out_weight,
    residual,
    mix_gain,
    routes,
    route_weights,
    expert_gate,
    expert_up,
    expert_down,
    final_gain,
):
    sp_n, tp_n = lax.axis_size("sp"), lax.axis_size("tp")
    tok, chan = glu_value.shape
    feat = final_gain.shape[0]
    width, ff = expert_gate.shape[1:]
    capacity = 4 * tok // sp_n
    y_n = tp_n // 2
    groups, most = len(SIZES), max(SIZES)
    rows = most * capacity
    wide = -(-tok // 128) * 128
    vmem = pl.BlockSpec(memory_space=pltpu.VMEM)
    hbm = pl.BlockSpec(memory_space=pl.ANY)
    dma = pltpu.SemaphoreType.DMA
    scratch = [
        pltpu.VMEM((tok, chan), BF16),
        pltpu.VMEM((tok, chan), BF16),
        pltpu.VMEM((1, tok), jnp.int32),
        pltpu.VMEM(conv_kernel.shape, BF16),
        pltpu.VMEM((1, chan), F32),
        pltpu.VMEM((1, width), F32),
        pltpu.VMEM((2, tok), jnp.int32),
        pltpu.VMEM((2, tok), F32),
        pltpu.VMEM((1, feat), F32),
        pltpu.VMEM((chan, width), BF16),
        pltpu.VMEM((tok, feat), BF16),
        pltpu.VMEM((width, ff), BF16),
        pltpu.VMEM((width, ff), BF16),
        pltpu.VMEM((ff, width), BF16),
        pltpu.VMEM((HALO, chan), BF16),
        pltpu.VMEM((HALO, chan), BF16),
        pltpu.VMEM((HALO, 128), jnp.int32),
        pltpu.VMEM((8, wide), F32),
        pltpu.VMEM((tok, 128), F32),
        pltpu.VMEM((HALO + tok, chan), F32),
        pltpu.VMEM((HALO + tok, 128), jnp.int32),
        pltpu.VMEM((tok, chan), F32),
        pltpu.VMEM((3, 8, wide), F32),
        pltpu.VMEM((3, tp_n, 8, wide), F32),
        pltpu.VMEM((y_n, tok, feat), BF16),
        pltpu.VMEM((y_n, tok, feat), BF16),
        pltpu.VMEM((y_n, tok, feat), BF16),
        pltpu.VMEM((y_n, tok, feat), BF16),
        pltpu.VMEM((tok, feat), F32),
        pltpu.VMEM((tok, feat), BF16),
        pltpu.VMEM((tok, feat), BF16),
        pltpu.VMEM((rows, width), BF16),
        pltpu.VMEM((sp_n, 8, 128), F32),
        pltpu.VMEM((sp_n, 8, 128), F32),
        pltpu.VMEM((sp_n, capacity, feat), BF16),
        pltpu.VMEM((tp_n, sp_n, capacity, feat), BF16),
        pltpu.VMEM((groups, rows, ff), BF16),
        pltpu.VMEM((groups, y_n, rows, feat), BF16),
        pltpu.VMEM((groups, y_n, rows, feat), BF16),
        pltpu.VMEM((groups, y_n, rows, feat), BF16),
        pltpu.VMEM((groups, y_n, rows, feat), BF16),
        pltpu.VMEM((groups, y_n, rows, feat), F32),
        pltpu.VMEM((sp_n, capacity, feat), BF16),
        pltpu.VMEM((sp_n, capacity, feat), BF16),
        dma((9,)),
        dma((5,)),
        dma((2, 2)),
        dma((3, tp_n)),
        dma((3, tp_n)),
        dma((2, y_n)),
        dma((2, y_n)),
        dma((sp_n,)),
        dma((sp_n,)),
        dma((sp_n,)),
        dma((sp_n,)),
        dma((2 * y_n - 1, sp_n)),
        dma((2 * y_n - 1, sp_n)),
        dma((groups, y_n)),
        dma((groups, y_n)),
        dma((groups, y_n, most)),
        dma((groups, y_n, most)),
        dma((sp_n,)),
        dma((sp_n,)),
    ]
    return pl.pallas_call(
        functools.partial(block_kernel, sp_n, tp_n, capacity, conv_kernel.shape[0]),
        out_shape=pltpu.VMEM((tok, feat), BF16),
        in_specs=[hbm] * 14,
        out_specs=vmem,
        scratch_shapes=scratch,
        compiler_params=pltpu.CompilerParams(
            collective_id=0, has_side_effects=True, vmem_limit_bytes=60 * 1024 * 1024
        ),
    )(
        glu_value,
        glu_gate,
        doc_ids[None, :],
        conv_kernel,
        conv_gain[None, :],
        out_weight,
        residual,
        mix_gain[None, :],
        routes.T,
        route_weights.T,
        expert_gate,
        expert_up,
        expert_down,
        final_gain[None, :],
    )


def local(*args):
    sp_n, tp_n = lax.axis_size("sp"), lax.axis_size("tp")
    tok, chan = args[0].shape
    ff = args[10].shape[2]
    feat = args[13].shape[0]
    aligned = (
        chan % 128 == 0
        and feat % TILE == 0
        and ff % TILE == 0
        and (4 * tok // sp_n) % 32 == 0
        and 4 * tok // sp_n <= 128
        and tok % HALO == 0
        and args[3].shape[0] <= HALO
        and tp_n % 2 == 0
        and tp_n > 2
        and sp_n == len(TURNS)
        and ff <= 2 * TILE * (len(PLAN[1]) - 2)
        and args[10].shape[0] == 1
    )
    return (local_kernel if aligned else local_plain)(*args)


def solution(mesh):
    return jax.shard_map(
        local,
        mesh=mesh,
        in_specs=(
            P("sp", "tp"),
            P("sp", "tp"),
            P("sp"),
            P(None, "tp"),
            P("tp"),
            P("tp", None),
            P("sp", None),
            P(),
            P("sp", None),
            P("sp", None),
            P("sp", None, "tp"),
            P("sp", None, "tp"),
            P("sp", "tp", None),
            P("tp"),
        ),
        out_specs=P("sp", "tp"),
        check_vma=False,
    )
```
